32 devices in a mesh: sp: 4 (over z), tp: 8 (over y, x, core).
Axes of the slice: x: 2, y: 2, z: 4, core: 2. Of those that a mesh axis runs over, the one named last changes fastest.
Arguments:
- activations: bfloat16 [1024, 2048], P('sp', 'tp'), may hold values from -170 to 170
- norm_gain: float32 [2048], replicated, may hold values from 0.1 to 1.9
- query_weight: bfloat16 [2048, 1536], P(None, 'tp'), may hold values from -0.125 to 0.125
- latent_weight: bfloat16 [2048, 512], P(None, 'tp'), may hold values from -0.125 to 0.125
- rope_key_weight: bfloat16 [2048, 64], replicated, may hold values from -0.125 to 0.125
- latent_gain: float32 [512], replicated, may hold values from 1.5 to 64
- expand_weight: bfloat16 [512, 2048], P(None, 'tp'), may hold values from -0.25 to 0.25
- gate_weight: bfloat16 [2048, 1024], P(None, 'tp'), may hold values from -0.125 to 0.125
- pre_weight: bfloat16 [2048, 1024], P(None, 'tp'), may hold values from -0.125 to 0.125
- value_weight: bfloat16 [2048, 1024], P(None, 'tp'), may hold values from -0.125 to 0.125
- conv_kernel: bfloat16 [3, 1024], P(None, 'tp'), may hold values from -3.5 to 3.5
- output_attend: bfloat16 [1024, 2048], P('tp'), may hold values from -0.1875 to 0.1875
- output_conv: bfloat16 [1024, 2048], P('tp'), may hold values from -0.125 to 0.125
Outputs:
- mixed: bfloat16 [1024, 2048], P(('sp', 'tp'))
- log_weight_sum: float32 [8, 1024], P('tp', 'sp')
The draws below stay inside these ranges and needn't reach their ends.
All inputs are finite; a program needn't handle non-finite values.
Results may differ from the reference program's by a relative error of at most 0.035.
The reference program's roundings to bfloat16 on the way count: a program that leaves them out, or rounds other values in their place, can miss the bound.
Values may be sent and summed in bfloat16 or wider, within the bound.
No kernel may reach another device: no remote copies, remote signals or barrier semaphores. Data moves between devices by JAX's collectives and lax.ppermute only.
A program may use at most 128 MiB of HBM per device.

```python
import math
import jax
import jax.numpy as jnp
from jax import lax

D = 2048
HEADS = 8
NOPE = 128
ROPE = 64
VDIM = 128
KV_RANK = 512
CONV_CH = 1024
KERNEL = 3
GRID_W = 64
TOKENS = 1024
N_TP = 8


def draw_activations(key, part):
    noise_key = jax.random.fold_in(key, 11)
    scale_key = jax.random.fold_in(key, 12)
    steps_along = jnp.arange(D, dtype=jnp.float32) / D
    noise = jnp.clip(jax.random.normal(noise_key, (TOKENS, D), jnp.float32), -5.0, 5.0)
    column_scale = 3.0 ** steps_along
    row_scale = jnp.exp(jax.random.uniform(scale_key, (TOKENS, 1), jnp.float32, 0.0, 1.1))
    return (noise * column_scale * row_scale).astype(jnp.bfloat16)


def draw_latent_gain(key, part):
    gain_key = jax.random.fold_in(key, 21)
    lower_end = math.log(1.5)
    upper_end = math.log(6.0)
    return jnp.exp(jax.random.uniform(gain_key, (KV_RANK,), jnp.float32, lower_end, upper_end))


def level_of(rng, extent, cuts, least, largest):
    loudness, own = 1.0, jax.random.fold_in(rng, 6)
    for position, parts in cuts:
        heights = jnp.exp(jax.random.uniform(jax.random.fold_in(own, position), (parts,), jnp.float32, least / len(cuts), largest / len(cuts)))
        loudness = loudness * jnp.repeat(heights, extent[position] // parts).reshape([-1 if axis == position else 1 for axis in range(len(extent))])
    return loudness


def scatter_about(stream_key, shape, deviation, limit, shards=(), kind=jnp.bfloat16):
    entries = deviation * jax.random.normal(stream_key, shape, jnp.float32)
    if shards:
        entries = entries * level_of(stream_key, shape, shards, -0.22, 0.18)
    return jnp.clip(entries, -limit, limit).astype(kind)


def setup_inputs(seed: int = 0) -> dict:
    key_of = jax.random.split(jax.random.key(seed), 14)
    activations = draw_activations(jax.random.fold_in(key_of[13], 71), 0)
    norm_gain = jnp.clip(1.0 + 0.18 * jax.random.normal(key_of[1], (D,), jnp.float32), 0.1, 1.9)
    query_weight = scatter_about(key_of[2], (D, HEADS * (NOPE + ROPE)), D ** -0.5, 0.125, ((1, 8),))
    latent_weight = scatter_about(key_of[3], (D, KV_RANK), D ** -0.5, 0.125, ((1, 8),))
    rope_key_weight = scatter_about(key_of[4], (D, ROPE), D ** -0.5, 0.125)
    latent_gain = draw_latent_gain(jax.random.fold_in(key_of[13], 71), 0)
    expand_weight = scatter_about(key_of[6], (KV_RANK, HEADS * (NOPE + VDIM)), KV_RANK ** -0.5, 0.25, ((1, 8),))
    gate_weight = scatter_about(key_of[7], (D, CONV_CH), D ** -0.5, 0.125, ((1, 8),))
    pre_weight = scatter_about(key_of[8], (D, CONV_CH), D ** -0.5, 0.125, ((1, 8),))
    value_weight = scatter_about(key_of[9], (D, CONV_CH), D ** -0.5, 0.125, ((1, 8),))
    conv_kernel = scatter_about(key_of[10], (KERNEL, CONV_CH), KERNEL ** -0.5, 3.5, ((1, 8),))
    output_attend = scatter_about(key_of[11], (HEADS * VDIM, D), (HEADS * VDIM) ** -0.5, 0.1875, ((0, 8),))
    output_conv = scatter_about(key_of[12], (CONV_CH, D), (2 * CONV_CH) ** -0.5, 0.125, ((0, 8),))
    return {"activations": activations, "norm_gain": norm_gain, "query_weight": query_weight, "latent_weight": latent_weight, "rope_key_weight": rope_key_weight, "latent_gain": latent_gain, "expand_weight": expand_weight, "gate_weight": gate_weight, "pre_weight": pre_weight, "value_weight": value_weight, "conv_kernel": conv_kernel, "output_attend": output_attend, "output_conv": output_conv}


EPSILON = 1e-06
ROPE_BASE = 10000.0

def rotate(inputs, grid_rows, grid_cols):
    quarter = inputs.shape[-1] // 4
    inverse = ROPE_BASE ** (-jnp.arange(quarter, dtype=jnp.float32) / quarter)
    row_angle = (grid_rows[:, None] * inverse)[:, None, :]
    col_angle = (grid_cols[:, None] * inverse)[:, None, :]
    part_one = inputs[..., :quarter]
    part_two = inputs[..., quarter:2 * quarter]
    part_three = inputs[..., 2 * quarter:3 * quarter]
    part_four = inputs[..., 3 * quarter:]
    return jnp.concatenate([part_one * jnp.cos(row_angle) - part_two * jnp.sin(row_angle), part_one * jnp.sin(row_angle) + part_two * jnp.cos(row_angle), part_three * jnp.cos(col_angle) - part_four * jnp.sin(col_angle), part_three * jnp.sin(col_angle) + part_four * jnp.cos(col_angle)], axis=-1)

def reference(activations, norm_gain, query_weight, latent_weight, rope_key_weight, latent_gain, expand_weight, gate_weight, pre_weight, value_weight, conv_kernel, output_attend, output_conv):
    inputs_f32 = activations.astype(jnp.float32)
    scaled = (inputs_f32 * norm_gain).astype(jnp.bfloat16)
    inv_rms = lax.rsqrt(lax.optimization_barrier(jnp.mean(inputs_f32 * inputs_f32, axis=1, keepdims=True)) + EPSILON)

    def project(weight):
        return jnp.dot(scaled, weight, preferred_element_type=jnp.float32) * inv_rms
    positions = jnp.arange(TOKENS, dtype=jnp.int32)
    grid_rows = (positions // GRID_W).astype(jnp.float32)
    grid_cols = (positions % GRID_W).astype(jnp.float32)
    query = project(query_weight).reshape(TOKENS, HEADS, NOPE + ROPE)
    query = jnp.concatenate([query[..., :NOPE], rotate(query[..., NOPE:], grid_rows, grid_cols)], axis=-1)
    query = (query * (NOPE + ROPE) ** (-0.5)).astype(jnp.bfloat16)
    latent_part = project(latent_weight).astype(jnp.bfloat16).astype(jnp.float32)
    latent = (latent_part * lax.rsqrt(lax.optimization_barrier(jnp.mean(latent_part * latent_part, axis=1, keepdims=True)) + EPSILON) * latent_gain).astype(jnp.bfloat16)
    expanded = jnp.dot(latent, expand_weight, preferred_element_type=jnp.float32).astype(jnp.bfloat16)
    expanded = expanded.reshape(TOKENS, HEADS, NOPE + VDIM)
    rope_key = rotate(project(rope_key_weight)[:, None, :], grid_rows, grid_cols)[:, 0].astype(jnp.bfloat16)
    key_nope = expanded[..., :NOPE].astype(jnp.float32)
    values = expanded[..., NOPE:].astype(jnp.float32)
    rope_f32 = rope_key.astype(jnp.float32)
    query_block = math.gcd(TOKENS, 512)
    query_blocks = query.reshape(TOKENS // query_block, query_block, HEADS, NOPE + ROPE)

    def attend(block):
        block_f32 = block.astype(jnp.float32)
        scores = jnp.einsum('thd,jhd->htj', block_f32[..., :NOPE], key_nope)
        scores = scores + jnp.einsum('thd,jd->htj', block_f32[..., NOPE:], rope_f32)
        row_max = lax.optimization_barrier(jnp.max(scores, axis=-1))
        shifted = jnp.exp(scores - row_max[..., None])
        row_sum = lax.optimization_barrier(jnp.sum(shifted, axis=-1))
        weights = lax.optimization_barrier(shifted.astype(jnp.bfloat16)).astype(jnp.float32)
        summed = jnp.einsum('htj,jhd->thd', weights, values)
        attended_block = (summed / row_sum.T[..., None]).astype(jnp.bfloat16)
        return (attended_block, row_max + jnp.log(row_sum))
    attended_blocks, log_blocks = lax.map(attend, query_blocks)
    attended = attended_blocks.reshape(TOKENS, HEADS * VDIM)
    log_weight_sum = jnp.transpose(log_blocks, (1, 0, 2)).reshape(HEADS, TOKENS)
    pre_mix = (project(pre_weight) * project(value_weight)).astype(jnp.bfloat16).astype(jnp.float32)
    padded = jnp.pad(pre_mix, ((1, 1), (0, 0)))
    kernel = conv_kernel.astype(jnp.float32)
    convolved = kernel[0] * padded[:-2] + kernel[1] * padded[1:-1] + kernel[2] * padded[2:]
    conv_mixed = (project(gate_weight) * convolved).astype(jnp.bfloat16)
    attend_cols = HEADS * VDIM // N_TP
    conv_cols = CONV_CH // N_TP
    summed_out = jnp.zeros((TOKENS, D), jnp.float32)
    for group_index in range(N_TP):
        head_part = attended[:, group_index * attend_cols:(group_index + 1) * attend_cols]
        chan_part = conv_mixed[:, group_index * conv_cols:(group_index + 1) * conv_cols]
        partial_value = jnp.dot(head_part, output_attend[group_index * attend_cols:(group_index + 1) * attend_cols], preferred_element_type=jnp.float32)
        partial_value = partial_value + jnp.dot(chan_part, output_conv[group_index * conv_cols:(group_index + 1) * conv_cols], preferred_element_type=jnp.float32)
        summed_out = summed_out + lax.optimization_barrier(partial_value.astype(jnp.bfloat16)).astype(jnp.float32)
    mixed = summed_out.astype(jnp.bfloat16)
    return (mixed, log_weight_sum)
```

```python
import functools

import jax
import jax.numpy as jnp
from jax import lax
from jax.experimental import pallas as pl
from jax.experimental.pallas import tpu as pltpu
from jax.sharding import PartitionSpec as P

NOPE = 128
ROPE = 64
VDIM = 128
GRID_W = 64
EPSILON = 1e-06
ROPE_BASE = 10000.0
LANES = 128
HALO = 16
F32 = jnp.float32
BF16 = jnp.bfloat16


def swap(array, axis, mask):
    peers = lax.axis_size(axis)
    return lax.ppermute(array, axis, [(i, i ^ mask) for i in range(peers)])


def kernel_call(body, outs, limit, scratch=(), flops=0, nbytes=0, name=None):
    whole = pl.BlockSpec(memory_space=pltpu.VMEM)

    def call(*operands):
        return pl.pallas_call(
            body,
            out_shape=[jax.ShapeDtypeStruct(shape, dtype) for shape, dtype in outs],
            in_specs=[whole] * len(operands),
            out_specs=[whole] * len(outs),
            scratch_shapes=list(scratch),
            compiler_params=pltpu.CompilerParams(vmem_limit_bytes=limit),
            cost_estimate=pl.CostEstimate(flops=flops, bytes_accessed=nbytes, transcendentals=0),
            name=name,
        )(*operands)

    return call


def rotation(positions):
    lane = jnp.arange(LANES) % ROPE
    quarter = ROPE // 4
    inverse = ROPE_BASE ** (-(lane % quarter).astype(F32) / quarter)
    rows = (positions // GRID_W).astype(F32)[:, None]
    cols = (positions % GRID_W).astype(F32)[:, None]
    angle = jnp.where(lane < 2 * quarter, rows, cols) * inverse
    sign = jnp.where((lane // quarter) % 2 == 0, -1.0, 1.0).astype(F32)
    return jnp.cos(angle), jnp.sin(angle) * sign


def rotate(values, cosines, sines):
    quarter = ROPE // 4
    lane = lax.broadcasted_iota(jnp.int32, values.shape, 1)
    first = (lane // quarter) % 2 == 0
    ahead = pltpu.roll(values, LANES - quarter, 1)
    behind = pltpu.roll(values, quarter, 1)
    return values * cosines + jnp.where(first, ahead, behind) * sines


def low_lanes(shape):
    return lax.broadcasted_iota(jnp.int32, shape, 1) < ROPE


def project_first(
    even_ref, odd_ref, gain_ref, key_w_ref, mix_w_ref, cos_ref, sin_ref,
    scaled_ref, inv_ref, message_ref, mix_ref, key_ref,
):
    rank = lax.axis_index("tp")
    pairs, tokens, width = even_ref.shape
    half = tokens // 2
    total = jnp.zeros((tokens, LANES), F32)
    for core, ref in ((0, even_ref), (1, odd_ref)):
        for i in range(pairs):
            owner = rank ^ (2 * i + core)
            piece = ref[i].astype(F32)
            squares = piece * piece
            for j in range(width // LANES):
                total = total + squares[:, j * LANES : (j + 1) * LANES]
            gain = gain_ref[pl.ds(owner, 1), :]
            start = pl.multiple_of(owner * width, width)
            scaled_ref[:, pl.ds(start, width)] = (piece * gain).astype(BF16)
    features = 2 * pairs * width
    inv = lax.rsqrt(jnp.sum(total, axis=1, keepdims=True) / features + EPSILON)
    inv_ref[...] = jnp.broadcast_to(inv, inv_ref.shape)
    scaled = scaled_ref[...]
    keys = jnp.dot(scaled, key_w_ref[...], preferred_element_type=F32) * inv
    mixes = jnp.dot(scaled, mix_w_ref[...], preferred_element_type=F32) * inv
    mix = (mixes[:, :LANES] * mixes[:, LANES:]).astype(BF16)
    mix_ref[...] = mix
    latent = keys[:, :LANES]
    low = low_lanes((half, LANES))
    message_ref[:half, :] = jnp.where(low, latent[:half], latent[half:]).astype(BF16)
    key_ref[...] = keys[:, LANES:]
    share = half // (2 * pairs)
    start = pl.multiple_of(rank * share, share)
    turned = []
    for base in (0, half):
        rows = pl.ds(start + base, share)
        turned.append(rotate(key_ref[rows, :], cos_ref[rows, :], sin_ref[rows, :]))
    low = low_lanes((share, LANES))
    message_ref[half : half + share, :] = jnp.where(low, turned[0], turned[1]).astype(BF16)
    row = lax.broadcasted_iota(jnp.int32, (HALO, LANES), 0)
    first = jnp.broadcast_to(mix[:1].astype(F32), (HALO, LANES))
    last = jnp.broadcast_to(mix[tokens - 1 :].astype(F32), (HALO, LANES))
    message_ref[half + share :, :] = jnp.where(row == 0, first, last).astype(BF16)


def project_second(
    scaled_ref, inv_ref, query_w_ref, gate_w_ref, cos_ref, sin_ref, query_ref, gate_ref
):
    scaled = scaled_ref[...]
    inv = inv_ref[...]
    scale = (NOPE + ROPE) ** (-0.5)
    query = jnp.dot(scaled, query_w_ref[...], preferred_element_type=F32)
    gate_ref[...] = jnp.dot(scaled, gate_w_ref[...], preferred_element_type=F32) * inv
    nope = (query[:, :NOPE] * inv * scale).astype(BF16)
    rope = rotate(query[:, NOPE:] * inv, cos_ref[...], sin_ref[...]) * scale
    low = low_lanes(rope.shape)
    query_ref[0, :, :NOPE] = nope
    query_ref[1, :, :NOPE] = nope
    query_ref[0, :, NOPE:] = jnp.where(low, rope, 0.0).astype(BF16)
    query_ref[1, :, NOPE:] = jnp.where(low, 0.0, rope).astype(BF16)


def attend(
    chunk, natural, even_ref, odd_ref, halo_ref, gain_ref, expand_ref, query_ref, gate_ref,
    mix_ref, taps_ref, keep_ref, send_ref, log_ref, latent_ref, rope_ref, both_ref,
):
    rank = lax.axis_index("tp")
    place = lax.axis_index("sp")
    pairs, blocks, _, _ = even_ref.shape
    ranks = 2 * pairs
    tokens = query_ref.shape[1]
    half = tokens // 2
    share = half // ranks
    entries = ranks * ROPE
    low = low_lanes((half, LANES))
    owned = [(rank ^ (2 * i + core), ref, i) for core, ref in ((0, even_ref), (1, odd_ref)) for i in range(pairs)]

    def one_chunk(first, state):
        scores, values = [], []
        for slot in range(chunk):
            block = first + slot
            total = jnp.zeros((half, LANES), F32)
            for owner, ref, i in owned:
                piece = ref[i, block, :half, :].astype(F32)
                total = total + piece * piece
                start = pl.multiple_of(owner * share, share)
                rope_ref[slot, pl.ds(start, share), :] = ref[i, block, half : half + share, :]
            sum_low = jnp.sum(jnp.where(low, total, 0.0), axis=1, keepdims=True)
            sum_high = jnp.sum(jnp.where(low, 0.0, total), axis=1, keepdims=True)
            inv = lax.rsqrt(jnp.where(low, sum_low, sum_high) / entries + EPSILON)
            for owner, ref, i in owned:
                piece = ref[i, block, :half, :].astype(F32)
                start = pl.multiple_of(owner * LANES, LANES)
                latent_ref[slot, :, pl.ds(start, LANES)] = (piece * inv * gain_ref[pl.ds(owner, 1), :]).astype(BF16)
        for slot in range(chunk):
            expanded = jnp.dot(latent_ref[slot], expand_ref[...], preferred_element_type=F32).astype(BF16)
            for side in range(2):
                base = side * (NOPE + VDIM)
                keys = jnp.concatenate([expanded[:, base : base + NOPE], rope_ref[slot]], axis=1)
                values.append(expanded[:, base + NOPE : base + NOPE + VDIM])
                scores.append(
                    lax.dot_general(query_ref[side], keys, (((1,), (1,)), ((), ())), preferred_element_type=F32)
                )
        peak = scores[0]
        for piece in scores[1:]:
            peak = jnp.maximum(peak, piece)
        peak = jnp.max(peak, axis=1, keepdims=True)
        if state is not None:
            peak = jnp.maximum(peak, state[0])
        total = jnp.zeros((tokens, LANES), F32)
        out = jnp.zeros((tokens, VDIM), F32)
        for piece, value in zip(scores, values, strict=True):
            weight = jnp.exp(piece - peak)
            total = total + weight
            out = out + jnp.dot(weight.astype(BF16), value, preferred_element_type=F32)
        total = jnp.sum(total, axis=1, keepdims=True)
        if state is not None:
            rescale = jnp.exp(state[0] - peak)
            total = total + state[1] * rescale
            out = out + state[2] * rescale
        return peak, total, out

    if blocks == chunk:
        peak, total, out = one_chunk(0, None)
    else:
        start = (
            jnp.full((tokens, 1), -jnp.inf, F32),
            jnp.zeros((tokens, 1), F32),
            jnp.zeros((tokens, VDIM), F32),
        )
        peak, total, out = lax.fori_loop(0, blocks // chunk, lambda i, state: one_chunk(i * chunk, state), start)
    both_ref[:, :VDIM] = out / total
    logs = jnp.broadcast_to(peak + jnp.log(total), (tokens, LANES))
    log_ref[...] = jnp.transpose(logs)[:1, :]

    mix = mix_ref[...].astype(F32)
    before_at = jnp.maximum(place - 1, 0)
    after_at = jnp.minimum(place + 1, blocks - 1)
    if not natural:
        before_at, after_at = before_at ^ place, after_at ^ place
    before = jnp.where(place > 0, halo_ref[before_at].astype(F32)[1:2, :], 0.0)
    after = jnp.where(place < blocks - 1, halo_ref[after_at].astype(F32)[0:1, :], 0.0)
    row = lax.broadcasted_iota(jnp.int32, mix.shape, 0)
    earlier = jnp.where(row == 0, before, pltpu.roll(mix, 1, 0))
    later = jnp.where(row == tokens - 1, after, pltpu.roll(mix, tokens - 1, 0))
    taps = taps_ref[...].astype(F32)
    convolved = taps[0:1] * earlier + taps[1:2] * mix + taps[2:3] * later
    both_ref[:, VDIM:] = gate_ref[...] * convolved

    chip, core = rank // 2, rank % 2
    rows = tokens // ranks
    for i in range(pairs):
        base = 2 * (chip ^ i)
        mine = pl.multiple_of((base + core) * rows, rows)
        other = pl.multiple_of((base + 1 - core) * rows, rows)
        keep_ref[i * rows : (i + 1) * rows, :] = both_ref[pl.ds(mine, rows), :].astype(BF16)
        send_ref[i * rows : (i + 1) * rows, :] = both_ref[pl.ds(other, rows), :].astype(BF16)


def output(keep_ref, got_ref, own_w_ref, other_w_ref, first_ref, *rest_refs):
    out = jnp.dot(keep_ref[...], own_w_ref[...], preferred_element_type=F32)
    out = out + jnp.dot(got_ref[...], other_w_ref[...], preferred_element_type=F32)
    rows = first_ref.shape[0]
    first_ref[...] = out[:rows]
    for i, ref in enumerate(rest_refs):
        ref[...] = out[(i + 1) * rows : (i + 2) * rows].astype(BF16)


def body(
    activations,
    norm_gain,
    query_weight,
    latent_weight,
    rope_key_weight,
    latent_gain,
    expand_weight,
    gate_weight,
    pre_weight,
    value_weight,
    conv_kernel,
    output_attend,
    output_conv,
):
    ranks = lax.axis_size("tp")
    places = lax.axis_size("sp")
    pairs = ranks // 2
    tokens, width = activations.shape
    features = ranks * width
    half = tokens // 2
    share = half // ranks
    rows = tokens // ranks
    channels = gate_weight.shape[1]

    gathered = [activations] + [swap(activations, "tp", 2 * i) for i in range(1, pairs)]
    even = jnp.stack(gathered)
    odd = swap(even, "tp", 1)
    own_w = jnp.concatenate([output_attend, output_conv], axis=0)
    other_w = swap(own_w, "tp", 1)

    key_w = jnp.concatenate([latent_weight, latent_weight, rope_key_weight, rope_key_weight], axis=1)
    mix_w = jnp.concatenate([pre_weight, value_weight], axis=1)
    query_w = jnp.concatenate([query_weight, query_weight[:, NOPE:]], axis=1)
    parts = expand_weight.reshape(ranks, 1, ROPE, 1, NOPE + VDIM)
    eye = jnp.eye(2, dtype=BF16).reshape(1, 2, 1, 2, 1)
    expand_w = (parts * eye).reshape(ranks * LANES, 2 * (NOPE + VDIM))
    gain = norm_gain.reshape(ranks, width)
    lat_gain = jnp.tile(latent_gain.reshape(ranks, ROPE), (1, 2))
    positions = lax.axis_index("sp") * tokens + jnp.arange(tokens, dtype=jnp.int32)
    cosines, sines = rotation(positions)

    message_rows = half + share + HALO
    scaled, inv, message, mix = kernel_call(
        project_first,
        [((tokens, features), BF16), ((tokens, LANES), F32), ((message_rows, LANES), BF16), ((tokens, channels), BF16)],
        12 << 20,
        scratch=[pltpu.VMEM((tokens, LANES), F32)],
        flops=2 * tokens * features * 4 * LANES,
        nbytes=4 * tokens * features,
        name="project_first",
    )(even, odd, gain, key_w, mix_w, cosines, sines)

    small = places <= 8 and places & (places - 1) == 0
    if small:
        around = [message] + [swap(message, "sp", i) for i in range(1, places)]
        around = jnp.stack(around)
    else:
        around = lax.all_gather(message, "sp", axis=0)
    query, gate = kernel_call(
        project_second,
        [((2, tokens, NOPE + LANES), BF16), ((tokens, channels), F32)],
        12 << 20,
        flops=2 * tokens * features * 3 * LANES,
        nbytes=4 * tokens * features,
        name="project_second",
    )(scaled, inv, query_w, gate_weight, cosines, sines)
    halo = around[:, half + share :, :]
    parts = around[:, : half + share, :]
    chip_even = jnp.stack([parts] + [swap(parts, "tp", 2 * i) for i in range(1, pairs)])
    chip_odd = swap(chip_even, "tp", 1)

    chunk = places if small else 4
    keep, send, logs = kernel_call(
        functools.partial(attend, chunk, not small),
        [((tokens // 2, VDIM + channels), BF16), ((tokens // 2, VDIM + channels), BF16), ((1, tokens), F32)],
        (16 << 20) if small else (60 << 20),
        scratch=[
            pltpu.VMEM((chunk, half, ranks * LANES), BF16),
            pltpu.VMEM((chunk, half, LANES), BF16),
            pltpu.VMEM((tokens, VDIM + channels), F32),
        ],
        flops=1 << 30,
        nbytes=1 << 22,
        name="attend",
    )(chip_even, chip_odd, halo, lat_gain, expand_w, query, gate, mix, conv_kernel)

    got = swap(send, "tp", 1)
    outs = kernel_call(
        output,
        [((rows, features), F32)] + [((rows, features), BF16)] * (pairs - 1),
        12 << 20,
        flops=1 << 28,
        nbytes=1 << 22,
        name="output",
    )(keep, got, own_w, other_w)
    total = outs[0]
    for i in range(1, pairs):
        total = total + swap(outs[i], "tp", 2 * i).astype(F32)
    return total.astype(BF16), logs


def solution(mesh):
    return jax.shard_map(
        body,
        mesh=mesh,
        in_specs=(
            P("sp", "tp"),
            P(),
            P(None, "tp"),
            P(None, "tp"),
            P(),
            P(),
            P(None, "tp"),
            P(None, "tp"),
            P(None, "tp"),
            P(None, "tp"),
            P(None, "tp"),
            P("tp", None),
            P("tp", None),
        ),
        out_specs=(P(("sp", "tp"), None), P("tp", "sp")),
        check_vma=False,
    )
```

```python
import functools
import math

import jax
import jax.numpy as jnp
from jax import lax
from jax.experimental import pallas as pl
from jax.experimental.pallas import tpu as pltpu
from jax.sharding import PartitionSpec as P

NOPE = 128
ROPE = 64
VDIM = 128
GRID_W = 64
EPSILON = 1e-06
ROPE_BASE = 10000.0
LANES = 128
HALO = 8
F32 = jnp.float32
BF16 = jnp.bfloat16


def swap(array, axis, mask):
    peers = lax.axis_size(axis)
    return lax.ppermute(array, axis, [(i, i ^ mask) for i in range(peers)])


def kernel_call(body, outs, limit, scratch=(), flops=0, nbytes=0, name=None):
    whole = pl.BlockSpec(memory_space=pltpu.VMEM)

    def call(*operands):
        return pl.pallas_call(
            body,
            out_shape=[jax.ShapeDtypeStruct(shape, dtype) for shape, dtype in outs],
            in_specs=[whole] * len(operands),
            out_specs=[whole] * len(outs),
            scratch_shapes=list(scratch),
            compiler_params=pltpu.CompilerParams(vmem_limit_bytes=limit),
            cost_estimate=pl.CostEstimate(flops=flops, bytes_accessed=nbytes, transcendentals=0),
            name=name,
        )(*operands)

    return call


def rotate(values, cosines, sines):
    quarter = ROPE // 4
    lane = lax.broadcasted_iota(jnp.int32, values.shape, 1)
    first = (lane // quarter) % 2 == 0
    ahead = pltpu.roll(values, LANES - quarter, 1)
    behind = pltpu.roll(values, quarter, 1)
    return values * cosines + jnp.where(first, ahead, behind) * sines


def low_lanes(shape):
    return lax.broadcasted_iota(jnp.int32, shape, 1) < ROPE


def prepare(
    latent_ref, rope_ref, query_ref, pre_ref, value_ref, expand_ref, gain_ref, attend_ref, conv_ref,
    key_w_ref, query_w_ref, mix_w_ref, expand_k_ref, expand_v_ref, lat_gain_ref, own_w_ref, cos_ref, sin_ref,
):
    own_w_ref[:VDIM, :] = attend_ref[...]
    own_w_ref[VDIM:, :] = conv_ref[...]
    for i in range(2):
        key_w_ref[i * ROPE : (i + 1) * ROPE, :] = latent_ref[...]
        key_w_ref[(i + 2) * ROPE : (i + 3) * ROPE, :] = rope_ref[...]
    query_w_ref[: NOPE + ROPE, :] = query_ref[...]
    query_w_ref[NOPE + ROPE :, :] = query_ref[NOPE:, :]
    mix_w_ref[:, :LANES] = pre_ref[...]
    mix_w_ref[:, LANES:] = value_ref[...]
    ranks = lat_gain_ref.shape[0]
    low = low_lanes((1, LANES))
    zeros = jnp.zeros((ROPE, LANES), BF16)
    for k in range(ranks):
        part = expand_ref[k * ROPE : (k + 1) * ROPE, :]
        upper = slice(k * LANES, k * LANES + ROPE)
        lower = slice(k * LANES + ROPE, (k + 1) * LANES)
        for ref, piece in ((expand_k_ref, part[:, :NOPE]), (expand_v_ref, part[:, NOPE:])):
            ref[upper, :LANES] = piece
            ref[upper, LANES:] = zeros
            ref[lower, :LANES] = zeros
            ref[lower, LANES:] = piece
        pair = gain_ref[:, (k // 2) * LANES : (k // 2 + 1) * LANES]
        turned = pltpu.roll(pair, ROPE, 1)
        chosen = (pair, turned) if k % 2 == 0 else (turned, pair)
        lat_gain_ref[k : k + 1, :] = jnp.where(low, *chosen)
    quarter = ROPE // 4
    groups = cos_ref.shape[0] // GRID_W
    first_row = lax.axis_index("sp") * groups

    def angles(rows, start):
        lane = lax.broadcasted_iota(jnp.int32, (rows, LANES), 1) % ROPE
        place = (lax.broadcasted_iota(jnp.int32, (rows, LANES), 0) + start).astype(F32)
        inverse = jnp.exp((lane % quarter).astype(F32) * (-math.log(ROPE_BASE) / quarter))
        angle = place * inverse
        sign = jnp.where((lane // quarter) % 2 == 0, -1.0, 1.0)
        return lane < 2 * quarter, jnp.cos(angle), jnp.sin(angle) * sign

    _, row_cos, row_sin = angles(groups, first_row)
    by_row, col_cos, col_sin = angles(GRID_W, 0)
    for g in range(groups):
        rows = slice(g * GRID_W, (g + 1) * GRID_W)
        cos_ref[rows, :] = jnp.where(by_row, row_cos[g : g + 1], col_cos)
        sin_ref[rows, :] = jnp.where(by_row, row_sin[g : g + 1], col_sin)


def dot_nt(left, right):
    return lax.dot_general(left, right, (((1,), (1,)), ((), ())), preferred_element_type=F32)


def project_first(pairs, *refs):
    pieces, refs = refs[: 2 * pairs], refs[2 * pairs :]
    gain_ref, key_w_ref, mix_w_ref, cos_ref, sin_ref = refs[:5]
    scaled_ref, inv_ref, message_ref, mix_ref, key_ref = refs[5:]
    rank = lax.axis_index("tp")
    tokens, width = pieces[0].shape
    half = tokens // 2
    total = jnp.zeros((tokens, LANES), F32)
    for i, ref in enumerate(pieces):
        owner = rank ^ (2 * (i % pairs) + i // pairs)
        piece = ref[...].astype(F32)
        squares = piece * piece
        for j in range(width // LANES):
            total = total + squares[:, j * LANES : (j + 1) * LANES]
        columns = pl.ds(pl.multiple_of(owner * width, width), width)
        scaled_ref[:, columns] = (piece * gain_ref[:, columns]).astype(BF16)
    features = 2 * pairs * width
    inv = lax.rsqrt(jnp.sum(total, axis=1, keepdims=True) / features + EPSILON)
    inv_ref[...] = jnp.broadcast_to(inv, inv_ref.shape)
    scaled = scaled_ref[...]
    keys = dot_nt(scaled, key_w_ref[...]) * inv
    mixes = jnp.dot(scaled, mix_w_ref[...], preferred_element_type=F32) * inv
    mix = (mixes[:, :LANES] * mixes[:, LANES:]).astype(BF16)
    mix_ref[...] = mix
    latent = keys[:, :LANES]
    low = low_lanes((half, LANES))
    message_ref[:half, :] = jnp.where(low, latent[:half], latent[half:]).astype(BF16)
    key_ref[...] = keys[:, LANES:]
    share = half // (2 * pairs)
    start = pl.multiple_of(rank * share, share)
    turned = []
    for base in (0, half):
        rows = pl.ds(start + base, share)
        turned.append(rotate(key_ref[rows, :], cos_ref[rows, :], sin_ref[rows, :]))
    low = low_lanes((share, LANES))
    message_ref[half : half + share, :] = jnp.where(low, turned[0], turned[1]).astype(BF16)
    row = lax.broadcasted_iota(jnp.int32, (HALO, LANES), 0)
    first = jnp.broadcast_to(mix[:1].astype(F32), (HALO, LANES))
    last = jnp.broadcast_to(mix[tokens - 1 :].astype(F32), (HALO, LANES))
    message_ref[half + share :, :] = jnp.where(row == 0, first, last).astype(BF16)


def project_second(
    scaled_ref, inv_ref, query_w_ref, gate_w_ref, cos_ref, sin_ref, query_ref, gate_ref
):
    scaled = scaled_ref[...]
    inv = inv_ref[...]
    scale = (NOPE + ROPE) ** (-0.5)
    query = dot_nt(scaled, query_w_ref[...])
    gate_ref[...] = jnp.dot(scaled, gate_w_ref[...], preferred_element_type=F32) * inv
    nope = (query[:, :NOPE] * inv * scale).astype(BF16)
    rope = rotate(query[:, NOPE:] * inv, cos_ref[...], sin_ref[...]) * scale
    low = low_lanes(rope.shape)
    query_ref[0, :, :NOPE] = nope
    query_ref[1, :, :NOPE] = nope
    query_ref[0, :, NOPE:] = jnp.where(low, rope, 0.0).astype(BF16)
    query_ref[1, :, NOPE:] = jnp.where(low, 0.0, rope).astype(BF16)


def attend(pairs, chunk, natural, *refs):
    pieces, refs = refs[: 2 * pairs], refs[2 * pairs :]
    gain_ref, expand_k_ref, expand_v_ref, query_ref, gate_ref, mix_ref, taps_ref = refs[:7]
    keep_ref, send_ref, log_ref, latent_ref, rope_ref, both_ref = refs[7:]
    rank = lax.axis_index("tp")
    place = lax.axis_index("sp")
    blocks = pieces[0].shape[0]
    ranks = 2 * pairs
    tokens = query_ref.shape[1]
    half = tokens // 2
    share = half // ranks
    entries = ranks * ROPE
    low = low_lanes((half, LANES))
    owned = [(rank ^ (2 * (i % pairs) + i // pairs), ref) for i, ref in enumerate(pieces)]

    def one_chunk(first, state):
        for slot in range(chunk):
            block = first + slot
            base = slot * half
            total = jnp.zeros((half, LANES), F32)
            for owner, ref in owned:
                piece = ref[block, :half, :].astype(F32)
                total = total + piece * piece
                start = pl.multiple_of(base + owner * share, share)
                rope_ref[pl.ds(start, share), :] = ref[block, half : half + share, :]
            sum_low = jnp.sum(jnp.where(low, total, 0.0), axis=1, keepdims=True)
            sum_high = jnp.sum(jnp.where(low, 0.0, total), axis=1, keepdims=True)
            inv = lax.rsqrt(jnp.where(low, sum_low, sum_high) / entries + EPSILON)
            for owner, ref in owned:
                piece = ref[block, :half, :].astype(F32)
                start = pl.multiple_of(owner * LANES, LANES)
                scaled = piece * inv * gain_ref[pl.ds(owner, 1), :]
                latent_ref[base : base + half, pl.ds(start, LANES)] = scaled.astype(BF16)
        latent = latent_ref[...]
        keys = jnp.dot(latent, expand_k_ref[...], preferred_element_type=F32).astype(BF16)
        values = lax.dot_general(
            expand_v_ref[...], latent, (((0,), (1,)), ((), ())), preferred_element_type=F32
        ).astype(BF16)
        rope = rope_ref[...]
        scores = [
            dot_nt(jnp.concatenate([keys[:, i * NOPE : (i + 1) * NOPE], rope], axis=1), query_ref[i])
            for i in range(2)
        ]
        peak = jnp.max(jnp.maximum(*scores), axis=0, keepdims=True)
        if state is not None:
            peak = jnp.maximum(peak, state[0])
        weights = [jnp.exp(piece - peak) for piece in scores]
        total = jnp.sum(weights[0] + weights[1], axis=0, keepdims=True)
        out = sum(
            jnp.dot(values[i * VDIM : (i + 1) * VDIM], weights[i].astype(BF16), preferred_element_type=F32)
            for i in range(2)
        )
        if state is not None:
            rescale = jnp.exp(state[0] - peak)
            total = total + state[1] * rescale
            out = out + state[2] * rescale
        return peak, total, out

    if blocks == chunk:
        peak, total, out = one_chunk(0, None)
    else:
        start = (
            jnp.full((1, tokens), -jnp.inf, F32),
            jnp.zeros((1, tokens), F32),
            jnp.zeros((VDIM, tokens), F32),
        )
        peak, total, out = lax.fori_loop(0, blocks // chunk, lambda i, state: one_chunk(i * chunk, state), start)
    both_ref[:, :VDIM] = jnp.transpose(out / total)
    log_ref[...] = peak + jnp.log(total)

    mix = mix_ref[...].astype(F32)
    before_at = jnp.maximum(place - 1, 0)
    after_at = jnp.minimum(place + 1, blocks - 1)
    if not natural:
        before_at, after_at = before_at ^ place, after_at ^ place
    edge = half + share
    before = jnp.where(place > 0, pieces[0][before_at, edge:, :].astype(F32)[1:2, :], 0.0)
    after = jnp.where(place < blocks - 1, pieces[0][after_at, edge:, :].astype(F32)[0:1, :], 0.0)
    row = lax.broadcasted_iota(jnp.int32, mix.shape, 0)
    earlier = jnp.where(row == 0, before, pltpu.roll(mix, 1, 0))
    later = jnp.where(row == tokens - 1, after, pltpu.roll(mix, tokens - 1, 0))
    taps = taps_ref[...].astype(F32)
    convolved = taps[0:1] * earlier + taps[1:2] * mix + taps[2:3] * later
    both_ref[:, VDIM:] = gate_ref[...] * convolved

    chip, core = rank // 2, rank % 2
    rows = tokens // ranks
    for i in range(pairs):
        base = 2 * (chip ^ i)
        mine = pl.multiple_of((base + core) * rows, rows)
        other = pl.multiple_of((base + 1 - core) * rows, rows)
        keep_ref[i * rows : (i + 1) * rows, :] = both_ref[pl.ds(mine, rows), :].astype(BF16)
        send_ref[i * rows : (i + 1) * rows, :] = both_ref[pl.ds(other, rows), :].astype(BF16)


def output(keep_ref, got_ref, own_w_ref, other_w_ref, first_ref, *rest_refs):
    out = jnp.dot(keep_ref[...], own_w_ref[...], preferred_element_type=F32)
    out = out + jnp.dot(got_ref[...], other_w_ref[...], preferred_element_type=F32)
    rows = first_ref.shape[0]
    first_ref[...] = out[:rows]
    for i, ref in enumerate(rest_refs):
        ref[...] = out[(i + 1) * rows : (i + 2) * rows].astype(BF16)


def body(
    activations,
    norm_gain,
    query_weight,
    latent_weight,
    rope_key_weight,
    latent_gain,
    expand_weight,
    gate_weight,
    pre_weight,
    value_weight,
    conv_kernel,
    output_attend,
    output_conv,
):
    ranks = lax.axis_size("tp")
    places = lax.axis_size("sp")
    pairs = ranks // 2
    tokens, width = activations.shape
    features = ranks * width
    half = tokens // 2
    share = half // ranks
    rows = tokens // ranks
    channels = gate_weight.shape[1]

    far = [swap(activations, "tp", 2 * i) for i in reversed(range(1, pairs))][::-1]
    even = [activations] + far
    odd = [swap(piece, "tp", 1) for piece in even]

    key_w, query_w, mix_w, expand_k, expand_v, lat_gain, own_w, cosines, sines = kernel_call(
        prepare,
        [
            ((4 * ROPE, features), BF16),
            ((NOPE + 2 * ROPE, features), BF16),
            ((features, 2 * LANES), BF16),
            ((ranks * LANES, 2 * NOPE), BF16),
            ((ranks * LANES, 2 * VDIM), BF16),
            ((ranks, LANES), F32),
            ((VDIM + channels, features), BF16),
            ((tokens, LANES), F32),
            ((tokens, LANES), F32),
        ],
        16 << 20,
        flops=1 << 28,
        nbytes=1 << 23,
        name="prepare",
    )(
        latent_weight.T, rope_key_weight.T, query_weight.T, pre_weight, value_weight, expand_weight,
        latent_gain.reshape(1, -1), output_attend, output_conv,
    )
    other_w = swap(own_w, "tp", 1)

    scaled, inv, message, mix = kernel_call(
        functools.partial(project_first, pairs),
        [
            ((tokens, features), BF16),
            ((tokens, LANES), F32),
            ((half + share + HALO, LANES), BF16),
            ((tokens, channels), BF16),
        ],
        12 << 20,
        scratch=[pltpu.VMEM((tokens, LANES), F32)],
        flops=2 * tokens * features * 4 * LANES,
        nbytes=4 * tokens * features,
        name="project_first",
    )(*even, *odd, norm_gain.reshape(1, -1), key_w, mix_w, cosines, sines)

    small = places <= 8 and places & (places - 1) == 0
    if small:
        around = [swap(message, "sp", i) for i in reversed(range(1, places))][::-1]
        around = jnp.stack([message] + around)
    else:
        around = lax.all_gather(message, "sp", axis=0)
    query, gate = kernel_call(
        project_second,
        [((2, tokens, NOPE + LANES), BF16), ((tokens, channels), F32)],
        12 << 20,
        flops=2 * tokens * features * 3 * LANES,
        nbytes=4 * tokens * features,
        name="project_second",
    )(scaled, inv, query_w, gate_weight, cosines, sines)
    chip_far = [swap(around, "tp", 2 * i) for i in reversed(range(1, pairs))][::-1]
    chip_even = [around] + chip_far
    chip_odd = [swap(piece, "tp", 1) for piece in chip_even]

    chunk = places if small else 4
    keep, send, logs = kernel_call(
        functools.partial(attend, pairs, chunk, not small),
        [((half, VDIM + channels), BF16), ((half, VDIM + channels), BF16), ((1, tokens), F32)],
        (16 << 20) if small else (60 << 20),
        scratch=[
            pltpu.VMEM((chunk * half, ranks * LANES), BF16),
            pltpu.VMEM((chunk * half, LANES), BF16),
            pltpu.VMEM((tokens, VDIM + channels), F32),
        ],
        flops=1 << 30,
        nbytes=1 << 22,
        name="attend",
    )(*chip_even, *chip_odd, lat_gain, expand_k, expand_v, query, gate, mix, conv_kernel)

    got = swap(send, "tp", 1)
    outs = kernel_call(
        output,
        [((rows, features), F32)] + [((rows, features), BF16)] * (pairs - 1),
        12 << 20,
        flops=1 << 28,
        nbytes=1 << 22,
        name="output",
    )(keep, got, own_w, other_w)
    arrived = [swap(outs[i], "tp", 2 * i) for i in reversed(range(1, pairs))]
    total = outs[0]
    for piece in arrived:
        total = total + piece.astype(F32)
    return total.astype(BF16), logs


def solution(mesh):
    return jax.shard_map(
        body,
        mesh=mesh,
        in_specs=(
            P("sp", "tp"),
            P(),
            P(None, "tp"),
            P(None, "tp"),
            P(),
            P(),
            P(None, "tp"),
            P(None, "tp"),
            P(None, "tp"),
            P(None, "tp"),
            P(None, "tp"),
            P("tp", None),
            P("tp", None),
        ),
        out_specs=(P(("sp", "tp"), None), P("tp", "sp")),
        check_vma=False,
    )
```

```python
import functools
import math

import jax
import jax.numpy as jnp
from jax import lax
from jax.experimental import pallas as pl
from jax.experimental.pallas import tpu as pltpu
from jax.sharding import PartitionSpec as P


NOPE = 128
ROPE = 64
VDIM = 128
GRID_W = 64
EPSILON = 1e-06
ROPE_BASE = 10000.0
LANES = 128
HALO = 8
F32 = jnp.float32
BF16 = jnp.bfloat16


def swap(array, axis, mask):
    peers = lax.axis_size(axis)
    return lax.ppermute(array, axis, [(i, i ^ mask) for i in range(peers)])


def exchange(array, axis, stride, peers):
    pieces = []
    for i in reversed(range(1, peers)):
        pieces.append(swap(array, axis, stride * i))
    return pieces[::-1]


def kernel_call(body, outs, limit, scratch=(), flops=0, nbytes=0, space=pltpu.VMEM):
    whole = pl.BlockSpec(memory_space=pltpu.VMEM)

    def call(*operands):
        if space is not pltpu.VMEM:
            operands = [pltpu.with_memory_space_constraint(operand, space) for operand in operands]
        return pl.pallas_call(
            body,
            out_shape=[jax.ShapeDtypeStruct(shape, dtype) for shape, dtype in outs],
            in_specs=[pl.BlockSpec(memory_space=space)] * len(operands),
            out_specs=[whole] * len(outs),
            scratch_shapes=list(scratch),
            compiler_params=pltpu.CompilerParams(vmem_limit_bytes=limit),
            cost_estimate=pl.CostEstimate(flops=flops, bytes_accessed=nbytes, transcendentals=0),
        )(*operands)

    return call


def rotate(values, cosines, sines):
    quarter = ROPE // 4
    lane = lax.broadcasted_iota(jnp.int32, values.shape, 1)
    first = (lane // quarter) % 2 == 0
    ahead = pltpu.roll(values, LANES - quarter, 1)
    behind = pltpu.roll(values, quarter, 1)
    return values * cosines + jnp.where(first, ahead, behind) * sines


def low_lanes(shape):
    return lax.broadcasted_iota(jnp.int32, shape, 1) < ROPE


def prepare(
    latent_ref, rope_ref, query_ref, pre_ref, value_ref, expand_ref, gain_ref, attend_ref, conv_ref, taps_ref,
    key_w_ref, query_w_ref, mix_w_ref, expand_k_ref, expand_v_ref, lat_gain_ref, own_w_ref, cos_ref, sin_ref,
    taps_out_ref, expand_in, gain_in, taps_in, sems,
):
    moves = [
        (expand_ref, expand_in),
        (gain_ref, gain_in),
        (taps_ref, taps_in),
        (latent_ref, key_w_ref.at[:ROPE]),
        (latent_ref, key_w_ref.at[ROPE : 2 * ROPE]),
        (rope_ref, key_w_ref.at[2 * ROPE : 3 * ROPE]),
        (rope_ref, key_w_ref.at[3 * ROPE :]),
        (pre_ref, mix_w_ref.at[:, :LANES]),
        (value_ref, mix_w_ref.at[:, LANES:]),
        (query_ref, query_w_ref.at[: NOPE + ROPE]),
        (query_ref.at[NOPE:], query_w_ref.at[NOPE + ROPE :]),
        (attend_ref, own_w_ref.at[:VDIM]),
        (conv_ref, own_w_ref.at[VDIM:]),
    ]
    copies = [pltpu.make_async_copy(source, target, sems.at[i]) for i, (source, target) in enumerate(moves)]
    for copy in copies:
        copy.start()
    quarter = ROPE // 4
    groups = cos_ref.shape[0] // GRID_W
    first_row = lax.axis_index("sp") * groups

    def angles(rows, start):
        lane = lax.broadcasted_iota(jnp.int32, (rows, LANES), 1) % ROPE
        place = (lax.broadcasted_iota(jnp.int32, (rows, LANES), 0) + start).astype(F32)
        inverse = jnp.exp((lane % quarter).astype(F32) * (-math.log(ROPE_BASE) / quarter))
        angle = place * inverse
        sign = jnp.where((lane // quarter) % 2 == 0, -1.0, 1.0)
        return lane < 2 * quarter, jnp.cos(angle), jnp.sin(angle) * sign

    _, row_cos, row_sin = angles(groups, first_row)
    by_row, col_cos, col_sin = angles(GRID_W, 0)
    for g in range(groups):
        rows = slice(g * GRID_W, (g + 1) * GRID_W)
        cos_ref[rows, :] = jnp.where(by_row, row_cos[g : g + 1], col_cos)
        sin_ref[rows, :] = jnp.where(by_row, row_sin[g : g + 1], col_sin)
    for copy in copies[:3]:
        copy.wait()
    taps_out_ref[...] = taps_in[...].astype(F32)
    ranks = lat_gain_ref.shape[0]
    low = low_lanes((1, LANES))
    zeros = jnp.zeros((ROPE, LANES), BF16)
    for k in range(ranks):
        part = expand_in[k * ROPE : (k + 1) * ROPE, :]
        upper = slice(k * LANES, k * LANES + ROPE)
        lower = slice(k * LANES + ROPE, (k + 1) * LANES)
        for ref, piece in ((expand_k_ref, part[:, :NOPE]), (expand_v_ref, part[:, NOPE:])):
            ref[upper, :LANES] = piece
            ref[upper, LANES:] = zeros
            ref[lower, :LANES] = zeros
            ref[lower, LANES:] = piece
        pair = gain_in[:, (k // 2) * LANES : (k // 2 + 1) * LANES]
        turned = pltpu.roll(pair, ROPE, 1)
        chosen = (pair, turned) if k % 2 == 0 else (turned, pair)
        lat_gain_ref[k : k + 1, :] = jnp.where(low, *chosen)
    for copy in copies[3:]:
        copy.wait()


def dot_nt(left, right):
    return lax.dot_general(left, right, (((1,), (1,)), ((), ())), preferred_element_type=F32)


def project_first(pairs, *refs):
    pieces, refs = refs[: 2 * pairs], refs[2 * pairs :]
    gain_ref, key_w_ref, mix_w_ref, cos_ref, sin_ref = refs[:5]
    scaled_ref, inv_ref, message_ref, mix_ref, key_ref = refs[5:]
    rank = lax.axis_index("tp")
    tokens, width = pieces[0].shape
    half = tokens // 2
    total = jnp.zeros((tokens, LANES), F32)
    for i, ref in enumerate(pieces):
        owner = rank ^ (2 * (i % pairs) + i // pairs)
        piece = ref[...].astype(F32)
        squares = piece * piece
        for j in range(width // LANES):
            total = total + squares[:, j * LANES : (j + 1) * LANES]
        columns = pl.ds(pl.multiple_of(owner * width, width), width)
        scaled_ref[:, columns] = (piece * gain_ref[:, columns]).astype(BF16)
    features = 2 * pairs * width
    inv = lax.rsqrt(jnp.sum(total, axis=1, keepdims=True) / features + EPSILON)
    inv_ref[...] = jnp.broadcast_to(inv, inv_ref.shape)
    scaled = scaled_ref[...]
    keys = dot_nt(scaled, key_w_ref[...]) * inv
    mixes = jnp.dot(scaled, mix_w_ref[...], preferred_element_type=F32) * inv
    mix = (mixes[:, :LANES] * mixes[:, LANES:]).astype(BF16)
    mix_ref[...] = mix
    latent = keys[:, :LANES]
    low = low_lanes((half, LANES))
    message_ref[:half, :] = jnp.where(low, latent[:half], latent[half:]).astype(BF16)
    key_ref[...] = keys[:, LANES:]
    share = half // (2 * pairs)
    start = pl.multiple_of(rank * share, share)
    turned = []
    for base in (0, half):
        rows = pl.ds(start + base, share)
        turned.append(rotate(key_ref[rows, :], cos_ref[rows, :], sin_ref[rows, :]))
    low = low_lanes((share, LANES))
    message_ref[half : half + share, :] = jnp.where(low, turned[0], turned[1]).astype(BF16)
    row = lax.broadcasted_iota(jnp.int32, (HALO, LANES), 0)
    first = jnp.broadcast_to(mix[:1].astype(F32), (HALO, LANES))
    last = jnp.broadcast_to(mix[tokens - 1 :].astype(F32), (HALO, LANES))
    message_ref[half + share :, :] = jnp.where(row == 0, first, last).astype(BF16)


def project_second(
    scaled_ref, inv_ref, query_w_ref, gate_w_ref, cos_ref, sin_ref, query_ref, gate_ref
):
    scaled = scaled_ref[...]
    inv = inv_ref[...]
    scale = (NOPE + ROPE) ** (-0.5)
    query = dot_nt(scaled, query_w_ref[...])
    gate_ref[...] = jnp.dot(scaled, gate_w_ref[...], preferred_element_type=F32) * inv
    nope = (query[:, :NOPE] * inv * scale).astype(BF16)
    rope = rotate(query[:, NOPE:] * inv, cos_ref[...], sin_ref[...]) * scale
    low = low_lanes(rope.shape)
    query_ref[0, :, :NOPE] = nope
    query_ref[1, :, :NOPE] = nope
    query_ref[0, :, NOPE:] = jnp.where(low, rope, 0.0).astype(BF16)
    query_ref[1, :, NOPE:] = jnp.where(low, 0.0, rope).astype(BF16)


def attend(pairs, chunk, natural, *refs):
    pieces, halos, refs = refs[: 2 * pairs], refs[2 * pairs : -13], refs[-13:]
    gain_ref, expand_k_ref, expand_v_ref, query_ref, gate_ref, mix_ref, taps_ref = refs[:7]
    keep_ref, send_ref, log_ref, latent_ref, rope_ref, both_ref = refs[7:]
    rank = lax.axis_index("tp")
    place = lax.axis_index("sp")
    blocks = pieces[0].shape[0]
    ranks = 2 * pairs
    tokens = query_ref.shape[1]
    half = tokens // 2
    share = half // ranks
    entries = ranks * ROPE
    low = low_lanes((half, LANES))
    owned = [(rank ^ (2 * (i % pairs) + i // pairs), ref) for i, ref in enumerate(pieces)]

    def one_chunk(first, state):
        for slot in range(chunk):
            block = first + slot
            base = slot * half
            total = jnp.zeros((half, LANES), F32)
            for owner, ref in owned:
                piece = ref[block, :half, :].astype(F32)
                total = total + piece * piece
                start = pl.multiple_of(base + owner * share, share)
                rope_ref[pl.ds(start, share), :] = ref[block, half : half + share, :]
            sum_low = jnp.sum(jnp.where(low, total, 0.0), axis=1, keepdims=True)
            sum_high = jnp.sum(jnp.where(low, 0.0, total), axis=1, keepdims=True)
            inv = lax.rsqrt(jnp.where(low, sum_low, sum_high) / entries + EPSILON)
            for owner, ref in owned:
                piece = ref[block, :half, :].astype(F32)
                start = pl.multiple_of(owner * LANES, LANES)
                scaled = piece * inv * gain_ref[pl.ds(owner, 1), :]
                latent_ref[base : base + half, pl.ds(start, LANES)] = scaled.astype(BF16)
        latent = latent_ref[...]
        keys = jnp.dot(latent, expand_k_ref[...], preferred_element_type=F32).astype(BF16)
        values = lax.dot_general(
            expand_v_ref[...], latent, (((0,), (1,)), ((), ())), preferred_element_type=F32
        ).astype(BF16)
        rope = rope_ref[...]
        scores = [
            dot_nt(jnp.concatenate([keys[:, i * NOPE : (i + 1) * NOPE], rope], axis=1), query_ref[i])
            for i in range(2)
        ]
        peak = jnp.max(jnp.maximum(*scores), axis=0, keepdims=True)
        if state is not None:
            peak = jnp.maximum(peak, state[0])
        weights = [jnp.exp(piece - peak) for piece in scores]
        total = jnp.sum(weights[0] + weights[1], axis=0, keepdims=True)
        out = sum(
            jnp.dot(values[i * VDIM : (i + 1) * VDIM], weights[i].astype(BF16), preferred_element_type=F32)
            for i in range(2)
        )
        if state is not None:
            rescale = jnp.exp(state[0] - peak)
            total = total + state[1] * rescale
            out = out + state[2] * rescale
        return peak, total, out

    if blocks == chunk:
        peak, total, out = one_chunk(0, None)
    else:
        start = (
            jnp.full((1, tokens), -jnp.inf, F32),
            jnp.zeros((1, tokens), F32),
            jnp.zeros((VDIM, tokens), F32),
        )
        peak, total, out = lax.fori_loop(0, blocks // chunk, lambda i, state: one_chunk(i * chunk, state), start)
    both_ref[:, :VDIM] = jnp.transpose(out / total)
    log_ref[...] = peak + jnp.log(total)

    mix = mix_ref[...].astype(F32)

    def edge_of(other, at):
        inside = (other >= 0) & (other < blocks)
        other = jnp.clip(other, 0, blocks - 1)
        if natural:
            edges = halos[0][other].astype(F32)
        else:
            edges = jnp.zeros((HALO, LANES), F32)
            for i, ref in enumerate(halos):
                edges = jnp.where((other ^ place) == i, ref[half + share :, :].astype(F32), edges)
        return jnp.where(inside, edges[at : at + 1, :], 0.0)

    before = edge_of(place - 1, 1)
    after = edge_of(place + 1, 0)
    row = lax.broadcasted_iota(jnp.int32, mix.shape, 0)
    earlier = jnp.where(row == 0, before, pltpu.roll(mix, 1, 0))
    later = jnp.where(row == tokens - 1, after, pltpu.roll(mix, tokens - 1, 0))
    taps = taps_ref[...]
    convolved = taps[0:1] * earlier + taps[1:2] * mix + taps[2:3] * later
    both_ref[:, VDIM:] = gate_ref[...] * convolved

    chip, core = rank // 2, rank % 2
    rows = tokens // ranks
    for i in range(pairs):
        base = 2 * (chip ^ i)
        mine = pl.multiple_of((base + core) * rows, rows)
        other = pl.multiple_of((base + 1 - core) * rows, rows)
        keep_ref[i * rows : (i + 1) * rows, :] = both_ref[pl.ds(mine, rows), :].astype(BF16)
        send_ref[i * rows : (i + 1) * rows, :] = both_ref[pl.ds(other, rows), :].astype(BF16)


def output(keep_ref, got_ref, own_w_ref, other_w_ref, first_ref, *rest_refs):
    out = jnp.dot(keep_ref[...], own_w_ref[...], preferred_element_type=F32)
    out = out + jnp.dot(got_ref[...], other_w_ref[...], preferred_element_type=F32)
    rows = first_ref.shape[0]
    first_ref[...] = out[:rows]
    for i, ref in enumerate(rest_refs):
        ref[...] = out[(i + 1) * rows : (i + 2) * rows].astype(BF16)


def body(
    activations,
    norm_gain,
    query_weight,
    latent_weight,
    rope_key_weight,
    latent_gain,
    expand_weight,
    gate_weight,
    pre_weight,
    value_weight,
    conv_kernel,
    output_attend,
    output_conv,
):
    ranks = lax.axis_size("tp")
    places = lax.axis_size("sp")
    pairs = ranks // 2
    tokens, width = activations.shape
    features = ranks * width
    half = tokens // 2
    share = half // ranks
    rows = tokens // ranks
    channels = gate_weight.shape[1]

    even = [activations] + exchange(activations, "tp", 2, pairs)
    odd = [swap(piece, "tp", 1) for piece in even]

    key_w, query_w, mix_w, expand_k, expand_v, lat_gain, own_w, cosines, sines, taps = kernel_call(
        prepare,
        [
            ((4 * ROPE, features), BF16),
            ((NOPE + 2 * ROPE, features), BF16),
            ((features, 2 * LANES), BF16),
            ((ranks * LANES, 2 * NOPE), BF16),
            ((ranks * LANES, 2 * VDIM), BF16),
            ((ranks, LANES), F32),
            ((VDIM + channels, features), BF16),
            ((tokens, LANES), F32),
            ((tokens, LANES), F32),
            (conv_kernel.shape, F32),
        ],
        16 << 20,
        scratch=[
            pltpu.VMEM(expand_weight.shape, BF16),
            pltpu.VMEM((1, latent_gain.shape[0]), F32),
            pltpu.VMEM(conv_kernel.shape, BF16),
            pltpu.SemaphoreType.DMA((13,)),
        ],
        space=pltpu.HBM,
        flops=1 << 28,
        nbytes=1 << 23,
    )(
        latent_weight.T, rope_key_weight.T, query_weight.T, pre_weight, value_weight, expand_weight,
        latent_gain.reshape(1, -1), output_attend, output_conv, conv_kernel,
    )
    other_w = swap(own_w, "tp", 1)

    scaled, inv, message, mix = kernel_call(
        functools.partial(project_first, pairs),
        [
            ((tokens, features), BF16),
            ((tokens, LANES), F32),
            ((half + share + HALO, LANES), BF16),
            ((tokens, channels), BF16),
        ],
        12 << 20,
        scratch=[pltpu.VMEM((tokens, LANES), F32)],
        flops=2 * tokens * features * 4 * LANES,
        nbytes=4 * tokens * features,
    )(*even, *odd, norm_gain.reshape(1, -1), key_w, mix_w, cosines, sines)

    small = places <= 8 and places & (places - 1) == 0
    if small:
        halos = [message] + exchange(message, "sp", 1, places)
        around = jnp.stack([piece[: half + share] for piece in halos])
    else:
        around = lax.all_gather(message, "sp", axis=0)
        around, halos = around[:, : half + share], [around[:, half + share :]]
    query, gate = kernel_call(
        project_second,
        [((2, tokens, NOPE + LANES), BF16), ((tokens, channels), F32)],
        12 << 20,
        flops=2 * tokens * features * 3 * LANES,
        nbytes=4 * tokens * features,
    )(scaled, inv, query_w, gate_weight, cosines, sines)
    chip_even = [around] + exchange(around, "tp", 2, pairs)
    chip_odd = [swap(piece, "tp", 1) for piece in chip_even]

    chunk = places if small else 4
    keep, send, logs = kernel_call(
        functools.partial(attend, pairs, chunk, not small),
        [((half, VDIM + channels), BF16), ((half, VDIM + channels), BF16), ((1, tokens), F32)],
        (16 << 20) if small else (60 << 20),
        scratch=[
            pltpu.VMEM((chunk * half, ranks * LANES), BF16),
            pltpu.VMEM((chunk * half, LANES), BF16),
            pltpu.VMEM((tokens, VDIM + channels), F32),
        ],
        flops=1 << 30,
        nbytes=1 << 22,
    )(*chip_even, *chip_odd, *halos, lat_gain, expand_k, expand_v, query, gate, mix, taps)

    got = swap(send, "tp", 1)
    outs = kernel_call(
        output,
        [((rows, features), F32)] + [((rows, features), BF16)] * (pairs - 1),
        12 << 20,
        flops=1 << 28,
        nbytes=1 << 22,
    )(keep, got, own_w, other_w)
    arrived = [swap(outs[i], "tp", 2 * i) for i in reversed(range(1, pairs))]
    total = outs[0]
    for piece in arrived:
        total = total + piece.astype(F32)
    return total.astype(BF16), logs


def solution(mesh):
    return jax.shard_map(
        body,
        mesh=mesh,
        in_specs=(
            P("sp", "tp"),
            P(),
            P(None, "tp"),
            P(None, "tp"),
            P(),
            P(),
            P(None, "tp"),
            P(None, "tp"),
            P(None, "tp"),
            P(None, "tp"),
            P(None, "tp"),
            P("tp", None),
            P("tp", None),
        ),
        out_specs=(P(("sp", "tp"), None), P("tp", "sp")),
        check_vma=False,
    )
```

```python
import functools
import math

import jax
import jax.numpy as jnp
from jax import lax
from jax.experimental import pallas as pl
from jax.experimental.pallas import tpu as pltpu
from jax.sharding import PartitionSpec as P


NOPE = 128
ROPE = 64
VDIM = 128
GRID_W = 64
EPSILON = 1e-06
ROPE_BASE = 10000.0
LANES = 128
HALO = 8
F32 = jnp.float32
BF16 = jnp.bfloat16


def swap(array, axis, mask):
    peers = lax.axis_size(axis)
    return lax.ppermute(array, axis, [(i, i ^ mask) for i in range(peers)])


def exchange(array, axis, stride, peers):
    pieces = []
    for i in reversed(range(1, peers)):
        pieces.append(swap(array, axis, stride * i))
    return pieces[::-1]


def swap_each(arrays):
    pieces = []
    for array in arrays:
        pieces.append(swap(array, "tp", 1))
    return pieces


def kernel_call(body, outs, limit, scratch=(), flops=0, nbytes=0, in_hbm=()):
    whole = pl.BlockSpec(memory_space=pltpu.VMEM)

    def call(*operands):
        spaces = [pltpu.HBM if i in in_hbm else pltpu.VMEM for i in range(len(operands))]
        operands = [
            pltpu.with_memory_space_constraint(operand, space) if space is pltpu.HBM else operand
            for operand, space in zip(operands, spaces, strict=True)
        ]
        return pl.pallas_call(
            body,
            out_shape=[jax.ShapeDtypeStruct(shape, dtype) for shape, dtype in outs],
            in_specs=[pl.BlockSpec(memory_space=space) for space in spaces],
            out_specs=[whole] * len(outs),
            scratch_shapes=list(scratch),
            compiler_params=pltpu.CompilerParams(vmem_limit_bytes=limit),
            cost_estimate=pl.CostEstimate(flops=flops, bytes_accessed=nbytes, transcendentals=0),
        )(*operands)

    return call


def rotate(values, cosines, sines):
    quarter = ROPE // 4
    lane = lax.broadcasted_iota(jnp.int32, values.shape, 1)
    first = (lane // quarter) % 2 == 0
    ahead = pltpu.roll(values, LANES - quarter, 1)
    behind = pltpu.roll(values, quarter, 1)
    return values * cosines + jnp.where(first, ahead, behind) * sines


def low_lanes(shape):
    return lax.broadcasted_iota(jnp.int32, shape, 1) < ROPE


def prepare(
    latent_ref, rope_ref, query_ref, pre_ref, value_ref, attend_ref, conv_ref, partner_ref,
    key_w_ref, query_w_ref, mix_w_ref, own_w_ref, cos_ref, sin_ref, sems,
):
    core = lax.axis_index("tp") % 2
    mine = pl.ds(pl.multiple_of(core * ROPE, ROPE), ROPE)
    moves = [
        (latent_ref, key_w_ref.at[mine]),
        (rope_ref, key_w_ref.at[2 * ROPE : 3 * ROPE]),
        (rope_ref, key_w_ref.at[3 * ROPE :]),
        (pre_ref, mix_w_ref.at[:, :LANES]),
        (value_ref, mix_w_ref.at[:, LANES:]),
        (query_ref, query_w_ref.at[: NOPE + ROPE]),
        (query_ref.at[NOPE:], query_w_ref.at[NOPE + ROPE :]),
        (attend_ref, own_w_ref.at[:VDIM]),
        (conv_ref, own_w_ref.at[VDIM:]),
    ]
    copies = [pltpu.make_async_copy(source, target, sems.at[i]) for i, (source, target) in enumerate(moves)]
    for copy in copies:
        copy.start()
    key_w_ref[pl.ds(pl.multiple_of((1 - core) * ROPE, ROPE), ROPE), :] = partner_ref[...]
    quarter = ROPE // 4
    groups = cos_ref.shape[0] // GRID_W
    first_row = lax.axis_index("sp") * groups

    def angles(rows, start):
        lane = lax.broadcasted_iota(jnp.int32, (rows, LANES), 1) % ROPE
        place = (lax.broadcasted_iota(jnp.int32, (rows, LANES), 0) + start).astype(F32)
        inverse = jnp.exp((lane % quarter).astype(F32) * (-math.log(ROPE_BASE) / quarter))
        angle = place * inverse
        sign = jnp.where((lane // quarter) % 2 == 0, -1.0, 1.0)
        return lane < 2 * quarter, jnp.cos(angle), jnp.sin(angle) * sign

    _, row_cos, row_sin = angles(groups, first_row)
    by_row, col_cos, col_sin = angles(GRID_W, 0)
    for g in range(groups):
        rows = slice(g * GRID_W, (g + 1) * GRID_W)
        cos_ref[rows, :] = jnp.where(by_row, row_cos[g : g + 1], col_cos)
        sin_ref[rows, :] = jnp.where(by_row, row_sin[g : g + 1], col_sin)
    for copy in copies:
        copy.wait()


def dot_nt(left, right):
    return lax.dot_general(left, right, (((1,), (1,)), ((), ())), preferred_element_type=F32)


def project_first(pairs, *refs):
    pieces, refs = refs[: 2 * pairs], refs[2 * pairs :]
    gain_ref, key_w_ref, mix_w_ref, cos_ref, sin_ref = refs[:5]
    scaled_ref, inv_ref, message_ref, mix_ref, key_ref = refs[5:]
    rank = lax.axis_index("tp")
    tokens, width = pieces[0].shape
    half = tokens // 2
    total = jnp.zeros((tokens, LANES), F32)
    for i, ref in enumerate(pieces):
        owner = rank ^ (2 * (i % pairs) + i // pairs)
        piece = ref[...].astype(F32)
        squares = piece * piece
        for j in range(width // LANES):
            total = total + squares[:, j * LANES : (j + 1) * LANES]
        columns = pl.ds(pl.multiple_of(owner * width, width), width)
        scaled_ref[:, columns] = (piece * gain_ref[:, columns]).astype(BF16)
    features = 2 * pairs * width
    inv = lax.rsqrt(jnp.sum(total, axis=1, keepdims=True) / features + EPSILON)
    inv_ref[...] = jnp.broadcast_to(inv, inv_ref.shape)
    scaled = scaled_ref[...]
    keys = dot_nt(scaled, key_w_ref[...]) * inv
    mixes = jnp.dot(scaled, mix_w_ref[...], preferred_element_type=F32) * inv
    mix = (mixes[:, :LANES] * mixes[:, LANES:]).astype(BF16)
    mix_ref[...] = mix
    key_ref[...] = keys
    chip, core = rank // 2, rank % 2
    start = pl.multiple_of(core * half, half)
    message_ref[:half, :] = key_ref[pl.ds(start, half), :LANES].astype(BF16)
    share = half // (2 * pairs)
    turned = []
    for base in (0, half // 2):
        rows = pl.ds(pl.multiple_of(start + base + chip * share, share), share)
        turned.append(rotate(key_ref[rows, LANES:], cos_ref[rows, :], sin_ref[rows, :]))
    low = low_lanes((share, LANES))
    message_ref[half : half + share, :] = jnp.where(low, turned[0], turned[1]).astype(BF16)
    row = lax.broadcasted_iota(jnp.int32, (HALO, LANES), 0)
    first = jnp.broadcast_to(mix[:1].astype(F32), (HALO, LANES))
    last = jnp.broadcast_to(mix[tokens - 1 :].astype(F32), (HALO, LANES))
    message_ref[half + share :, :] = jnp.where(row == 0, first, last).astype(BF16)


def project_second(natural, *refs):
    scaled_ref, inv_ref, query_w_ref, gate_w_ref, cos_ref, sin_ref, mix_ref, taps_ref = refs[:8]
    halos, (query_ref, conv_ref) = refs[8:-2], refs[-2:]
    scaled = scaled_ref[...]
    inv = inv_ref[...]
    scale = (NOPE + ROPE) ** (-0.5)
    query = dot_nt(scaled, query_w_ref[...])
    nope = (query[:, :NOPE] * inv * scale).astype(BF16)
    rope = rotate(query[:, NOPE:] * inv, cos_ref[...], sin_ref[...]) * scale
    low = low_lanes(rope.shape)
    query_ref[0, :, :NOPE] = nope
    query_ref[1, :, :NOPE] = nope
    query_ref[0, :, NOPE:] = jnp.where(low, rope, 0.0).astype(BF16)
    query_ref[1, :, NOPE:] = jnp.where(low, 0.0, rope).astype(BF16)

    gate = jnp.dot(scaled, gate_w_ref[...], preferred_element_type=F32) * inv
    mix = mix_ref[...].astype(F32)
    tokens = mix.shape[0]
    place, places = lax.axis_index("sp"), lax.axis_size("sp")

    def edge_of(other, at):
        inside = (other >= 0) & (other < places)
        other = jnp.clip(other, 0, places - 1)
        if natural:
            edges = halos[0][other].astype(F32)
        else:
            edges = jnp.zeros((HALO, LANES), F32)
            for i, ref in enumerate(halos):
                edges = jnp.where((other ^ place) == i, ref[ref.shape[0] - HALO :, :].astype(F32), edges)
        return jnp.where(inside, edges[at : at + 1, :], 0.0)

    row = lax.broadcasted_iota(jnp.int32, mix.shape, 0)
    earlier = jnp.where(row == 0, edge_of(place - 1, 1), pltpu.roll(mix, 1, 0))
    later = jnp.where(row == tokens - 1, edge_of(place + 1, 0), pltpu.roll(mix, tokens - 1, 0))
    taps = taps_ref[...].astype(F32)
    convolved = taps[0:1] * earlier + taps[1:2] * mix + taps[2:3] * later
    conv_ref[...] = (gate * convolved).astype(BF16)


def attend(slots, chunk, last, *refs):
    inputs = 1 + max(place for chip_slots in slots for place, _ in chip_slots)
    pieces, refs = refs[:inputs], refs[inputs:]
    gain_ref, expand_ref, query_ref = refs[:3]
    refs = refs[3:]
    if last:
        stats_in, out_in, conv_ref, keep_ref, send_ref, log_ref = refs[:6]
    else:
        stats_ref, out_ref = refs[:2]
    latent_ref, rope_ref = refs[-2:]
    rank = lax.axis_index("tp")
    chip, core = rank // 2, rank % 2
    pairs = len(slots)
    tokens = query_ref.shape[1]
    half = tokens // 2
    group = half // 2
    share = group // pairs
    entries = pairs * LANES

    views = [(chip ^ i, chip_slots) for i, chip_slots in enumerate(slots)]

    def rows_of(chip_slots, slot, first, start, count):
        place, at = chip_slots[slot if first is None else 0]
        at = at if first is None else first + slot
        rows = slice(start, start + count)
        return pieces[place][rows, :] if at is None else pieces[place][at, rows, :]

    def one_chunk(first, state):
        for slot in range(chunk):
            total = jnp.zeros((half, LANES), F32)
            for owner, chip_slots in views:
                piece = rows_of(chip_slots, slot, first, 0, half).astype(F32)
                total = total + piece * piece
                start = pl.multiple_of(slot * group + owner * share, share)
                rope_ref[pl.ds(start, share), :] = rows_of(chip_slots, slot, first, half, share)
            inv = lax.rsqrt(jnp.sum(total, axis=1, keepdims=True) / entries + EPSILON)
            for owner, chip_slots in views:
                piece = rows_of(chip_slots, slot, first, 0, half).astype(F32)
                columns = pl.ds(pl.multiple_of(owner * LANES, LANES), LANES)
                scaled = (piece * inv * gain_ref[:, columns]).astype(BF16)
                for side in range(2):
                    base = (side * chunk + slot) * group
                    latent_ref[base : base + group, columns] = scaled[side * group : (side + 1) * group]
        latent = latent_ref[...]
        keys = jnp.dot(latent, expand_ref[:, :NOPE], preferred_element_type=F32).astype(BF16)
        values = lax.dot_general(
            expand_ref[:, NOPE:], latent, (((0,), (1,)), ((), ())), preferred_element_type=F32
        ).astype(BF16)
        rope = rope_ref[...]
        count = chunk * group
        scores = [
            dot_nt(jnp.concatenate([keys[i * count : (i + 1) * count], rope], axis=1), query_ref[i])
            for i in range(2)
        ]
        peak = jnp.max(jnp.maximum(*scores), axis=0, keepdims=True)
        if state is not None:
            peak = jnp.maximum(peak, state[0])
        weights = [jnp.exp(piece - peak) for piece in scores]
        total = jnp.sum(weights[0] + weights[1], axis=0, keepdims=True)
        out = sum(
            jnp.dot(values[:, i * count : (i + 1) * count], weights[i].astype(BF16), preferred_element_type=F32)
            for i in range(2)
        )
        if state is not None:
            rescale = jnp.exp(state[0] - peak)
            total = total + state[1] * rescale
            out = out + state[2] * rescale
        return peak, total, out

    state = (stats_in[0:1], stats_in[1:2], out_in[...]) if last else None
    if chunk == len(views[0][1]):
        peak, total, out = one_chunk(None, state)
    else:
        if state is None:
            state = (
                jnp.full((1, tokens), -jnp.inf, F32),
                jnp.zeros((1, tokens), F32),
                jnp.zeros((VDIM, tokens), F32),
            )
        steps = len(views[0][1]) // chunk
        peak, total, out = lax.fori_loop(0, steps, lambda i, state: one_chunk(i * chunk, state), state)
    if not last:
        stats_ref[0:1] = peak
        stats_ref[1:2] = total
        out_ref[...] = out
        return
    log_ref[...] = peak + jnp.log(total)
    attended = jnp.transpose(out / total)
    rows = tokens // (2 * pairs)
    attend_ref = refs[-3]
    attend_ref[...] = attended.astype(BF16)
    for i in range(pairs):
        base = 2 * (chip ^ i)
        for ref, at in ((keep_ref, base + core), (send_ref, base + 1 - core)):
            source = pl.ds(pl.multiple_of(at * rows, rows), rows)
            ref[i * rows : (i + 1) * rows, :VDIM] = attend_ref[source, :]
            ref[i * rows : (i + 1) * rows, VDIM:] = conv_ref[source, :]


def output(keep_ref, got_ref, own_w_ref, other_w_ref, first_ref, *rest_refs):
    out = jnp.dot(keep_ref[...], own_w_ref[...], preferred_element_type=F32)
    out = out + jnp.dot(got_ref[...], other_w_ref[...], preferred_element_type=F32)
    rows = first_ref.shape[0]
    first_ref[...] = out[:rows]
    for i, ref in enumerate(rest_refs):
        ref[...] = out[(i + 1) * rows : (i + 2) * rows].astype(BF16)


def body(
    activations,
    norm_gain,
    query_weight,
    latent_weight,
    rope_key_weight,
    latent_gain,
    expand_weight,
    gate_weight,
    pre_weight,
    value_weight,
    conv_kernel,
    output_attend,
    output_conv,
):
    ranks = lax.axis_size("tp")
    places = lax.axis_size("sp")
    pairs = ranks // 2
    tokens, width = activations.shape
    features = ranks * width
    half = tokens // 2
    share = half // ranks
    rows = tokens // ranks
    channels = gate_weight.shape[1]

    even = [activations] + exchange(activations, "tp", 2, pairs)
    odd = swap_each(even)

    latent_t = latent_weight.T
    partner_t = swap(latent_t, "tp", 1)
    key_w, query_w, mix_w, own_w, cosines, sines = kernel_call(
        prepare,
        [
            ((4 * ROPE, features), BF16),
            ((NOPE + 2 * ROPE, features), BF16),
            ((features, 2 * LANES), BF16),
            ((VDIM + channels, features), BF16),
            ((tokens, LANES), F32),
            ((tokens, LANES), F32),
        ],
        16 << 20,
        scratch=[pltpu.SemaphoreType.DMA((9,))],
        flops=1 << 28,
        nbytes=1 << 23,
        in_hbm=range(7),
    )(
        latent_t, rope_key_weight.T, query_weight.T, pre_weight, value_weight, output_attend, output_conv,
        partner_t,
    )
    other_w = swap(own_w, "tp", 1)

    scaled, inv, message, mix = kernel_call(
        functools.partial(project_first, pairs),
        [
            ((tokens, features), BF16),
            ((tokens, LANES), F32),
            ((half + share + HALO, LANES), BF16),
            ((tokens, channels), BF16),
        ],
        12 << 20,
        scratch=[pltpu.VMEM((tokens, 2 * LANES), F32)],
        flops=2 * tokens * features * 4 * LANES,
        nbytes=4 * tokens * features,
    )(*even, *odd, norm_gain.reshape(1, -1), key_w, mix_w, cosines, sines)

    small = places <= 8 and places & (places - 1) == 0
    if small:
        halos = [message] + exchange(message, "sp", 1, places)
        near = message[: half + share]
        nears = [near] + exchange(near, "tp", 2, pairs)
        near_other = swap(jnp.stack(nears), "tp", 1)
        around = jnp.stack([piece[: half + share] for piece in halos[1:]])
    else:
        around = lax.all_gather(message, "sp", axis=0)
        around, halos = around[:, : half + share], [around[:, half + share :]]
    arounds = [around] + exchange(around, "tp", 2, pairs)
    others = swap_each(arounds)
    blocks = range(places - 1) if small else range(places)
    slots = [[(i, k) for k in blocks] for i in range(pairs)]
    other_slots = slots
    if small:
        other_slots = [[(pairs, i)] + chip_slots for i, chip_slots in enumerate(slots)]
        slots = [[(pairs + i, None)] + chip_slots for i, chip_slots in enumerate(slots)]
        arounds += nears
        others.append(near_other)

    query, conv = kernel_call(
        functools.partial(project_second, not small),
        [((2, tokens, NOPE + LANES), BF16), ((tokens, channels), BF16)],
        12 << 20,
        flops=2 * tokens * features * 3 * LANES,
        nbytes=4 * tokens * features,
    )(scaled, inv, query_w, gate_weight, cosines, sines, mix, conv_kernel, *halos)

    chunk = places if small else 4

    def attend_to(arrays, slots, last, outs, *operands):
        scratch = [
            pltpu.VMEM((tokens, VDIM), BF16),
            pltpu.VMEM((chunk * half, pairs * LANES), BF16),
            pltpu.VMEM((chunk * half // 2, LANES), BF16),
        ]
        return kernel_call(
            functools.partial(attend, slots, chunk, last),
            outs,
            (12 << 20) if small else (40 << 20),
            scratch=scratch if last else scratch[1:],
            flops=1 << 29,
            nbytes=1 << 22,
        )(*arrays, latent_gain.reshape(1, -1), expand_weight, query, *operands)

    stats, out = attend_to(arounds, slots, False, [((8, tokens), F32), ((VDIM, tokens), F32)])
    keep, send, logs = attend_to(
        others,
        other_slots,
        True,
        [((half, VDIM + channels), BF16), ((half, VDIM + channels), BF16), ((1, tokens), F32)],
        stats,
        out,
        conv,
    )

    got = swap(send, "tp", 1)
    outs = kernel_call(
        output,
        [((rows, features), F32)] + [((rows, features), BF16)] * (pairs - 1),
        12 << 20,
        flops=1 << 28,
        nbytes=1 << 22,
    )(keep, got, own_w, other_w)
    arrived = [swap(outs[i], "tp", 2 * i) for i in reversed(range(1, pairs))]
    total = outs[0]
    for piece in arrived:
        total = total + piece.astype(F32)
    return total.astype(BF16), logs


def solution(mesh):
    return jax.shard_map(
        body,
        mesh=mesh,
        in_specs=(
            P("sp", "tp"),
            P(),
            P(None, "tp"),
            P(None, "tp"),
            P(),
            P(),
            P(None, "tp"),
            P(None, "tp"),
            P(None, "tp"),
            P(None, "tp"),
            P(None, "tp"),
            P("tp", None),
            P("tp", None),
        ),
        out_specs=(P(("sp", "tp"), None), P("tp", "sp")),
        check_vma=False,
    )
```

```python
import functools
import math

import jax
import jax.numpy as jnp
from jax import lax
from jax.experimental import pallas as pl
from jax.experimental.pallas import tpu as pltpu
from jax.sharding import PartitionSpec as P


NOPE = 128
ROPE = 64
VDIM = 128
GRID_W = 64
EPSILON = 1e-06
ROPE_BASE = 10000.0
LANES = 128
HALO = 8
F32 = jnp.float32
BF16 = jnp.bfloat16


def swap(array, axis, mask):
    peers = lax.axis_size(axis)
    return lax.ppermute(array, axis, [(i, i ^ mask) for i in range(peers)])


def exchange(array, axis, stride, peers):
    pieces = []
    for i in reversed(range(1, peers)):
        pieces.append(swap(array, axis, stride * i))
    return pieces[::-1]


def swap_each(arrays):
    pieces = []
    for array in arrays:
        pieces.append(swap(array, "tp", 1))
    return pieces


def exchange_blocks(blocks):
    arrived = []
    for i in reversed(range(1, len(blocks))):
        arrived.append(swap(blocks[i], "tp", 2 * i))
    return arrived


def kernel_call(body, outs, limit, scratch=(), flops=0, nbytes=0, in_hbm=()):
    whole = pl.BlockSpec(memory_space=pltpu.VMEM)

    def call(*operands):
        spaces = [pltpu.HBM if i in in_hbm else pltpu.VMEM for i in range(len(operands))]
        operands = [
            pltpu.with_memory_space_constraint(operand, space) if space is pltpu.HBM else operand
            for operand, space in zip(operands, spaces, strict=True)
        ]
        return pl.pallas_call(
            body,
            out_shape=[jax.ShapeDtypeStruct(shape, dtype) for shape, dtype in outs],
            in_specs=[pl.BlockSpec(memory_space=space) for space in spaces],
            out_specs=[whole] * len(outs),
            scratch_shapes=list(scratch),
            compiler_params=pltpu.CompilerParams(vmem_limit_bytes=limit),
            cost_estimate=pl.CostEstimate(flops=flops, bytes_accessed=nbytes, transcendentals=0),
        )(*operands)

    return call


def rotate(values, cosines, sines):
    quarter = ROPE // 4
    lane = lax.broadcasted_iota(jnp.int32, values.shape, 1)
    first = (lane // quarter) % 2 == 0
    ahead = pltpu.roll(values, LANES - quarter, 1)
    behind = pltpu.roll(values, quarter, 1)
    return values * cosines + jnp.where(first, ahead, behind) * sines


def low_lanes(shape):
    return lax.broadcasted_iota(jnp.int32, shape, 1) < ROPE


def prepare(
    latent_ref, rope_ref, query_ref, pre_ref, value_ref, attend_ref, conv_ref, partner_ref,
    key_w_ref, query_w_ref, mix_w_ref, own_w_ref, cos_ref, sin_ref, sems,
):
    core = lax.axis_index("tp") % 2
    mine = pl.ds(pl.multiple_of(core * ROPE, ROPE), ROPE)
    moves = [
        (latent_ref, key_w_ref.at[mine]),
        (rope_ref, key_w_ref.at[2 * ROPE : 3 * ROPE]),
        (rope_ref, key_w_ref.at[3 * ROPE :]),
        (pre_ref, mix_w_ref.at[:, :LANES]),
        (value_ref, mix_w_ref.at[:, LANES:]),
        (query_ref, query_w_ref.at[: NOPE + ROPE]),
        (query_ref.at[NOPE:], query_w_ref.at[NOPE + ROPE :]),
        (attend_ref, own_w_ref.at[:VDIM]),
        (conv_ref, own_w_ref.at[VDIM:]),
    ]
    copies = [pltpu.make_async_copy(source, target, sems.at[i]) for i, (source, target) in enumerate(moves)]
    for copy in copies:
        copy.start()
    key_w_ref[pl.ds(pl.multiple_of((1 - core) * ROPE, ROPE), ROPE), :] = partner_ref[...]
    quarter = ROPE // 4
    groups = cos_ref.shape[0] // GRID_W
    first_row = lax.axis_index("sp") * groups

    def angles(rows, start):
        lane = lax.broadcasted_iota(jnp.int32, (rows, LANES), 1) % ROPE
        place = (lax.broadcasted_iota(jnp.int32, (rows, LANES), 0) + start).astype(F32)
        inverse = jnp.exp((lane % quarter).astype(F32) * (-math.log(ROPE_BASE) / quarter))
        angle = place * inverse
        sign = jnp.where((lane // quarter) % 2 == 0, -1.0, 1.0)
        return lane < 2 * quarter, jnp.cos(angle), jnp.sin(angle) * sign

    _, row_cos, row_sin = angles(groups, first_row)
    by_row, col_cos, col_sin = angles(GRID_W, 0)
    for g in range(groups):
        rows = slice(g * GRID_W, (g + 1) * GRID_W)
        cos_ref[rows, :] = jnp.where(by_row, row_cos[g : g + 1], col_cos)
        sin_ref[rows, :] = jnp.where(by_row, row_sin[g : g + 1], col_sin)
    for copy in copies:
        copy.wait()


def dot_nt(left, right):
    return lax.dot_general(left, right, (((1,), (1,)), ((), ())), preferred_element_type=F32)


def project_first(pairs, *refs):
    pieces, refs = refs[: 2 * pairs], refs[2 * pairs :]
    gain_ref, key_w_ref, mix_w_ref, cos_ref, sin_ref = refs[:5]
    scaled_ref, inv_ref, message_ref, mix_ref, key_ref = refs[5:]
    rank = lax.axis_index("tp")
    tokens, width = pieces[0].shape
    half = tokens // 2
    total = jnp.zeros((tokens, LANES), F32)
    for i, ref in enumerate(pieces):
        owner = rank ^ (2 * (i % pairs) + i // pairs)
        piece = ref[...].astype(F32)
        squares = piece * piece
        for j in range(width // LANES):
            total = total + squares[:, j * LANES : (j + 1) * LANES]
        columns = pl.ds(pl.multiple_of(owner * width, width), width)
        scaled_ref[:, columns] = (piece * gain_ref[:, columns]).astype(BF16)
    features = 2 * pairs * width
    inv = lax.rsqrt(jnp.sum(total, axis=1, keepdims=True) / features + EPSILON)
    inv_ref[...] = jnp.broadcast_to(inv, inv_ref.shape)
    scaled = scaled_ref[...]
    keys = dot_nt(scaled, key_w_ref[...]) * inv
    mixes = jnp.dot(scaled, mix_w_ref[...], preferred_element_type=F32) * inv
    mix = (mixes[:, :LANES] * mixes[:, LANES:]).astype(BF16)
    mix_ref[...] = mix
    key_ref[...] = keys
    chip, core = rank // 2, rank % 2
    start = pl.multiple_of(core * half, half)
    message_ref[:half, :] = key_ref[pl.ds(start, half), :LANES].astype(BF16)
    share = half // (2 * pairs)
    turned = []
    for base in (0, half // 2):
        rows = pl.ds(pl.multiple_of(start + base + chip * share, share), share)
        turned.append(rotate(key_ref[rows, LANES:], cos_ref[rows, :], sin_ref[rows, :]))
    low = low_lanes((share, LANES))
    message_ref[half : half + share, :] = jnp.where(low, turned[0], turned[1]).astype(BF16)
    row = lax.broadcasted_iota(jnp.int32, (HALO, LANES), 0)
    first = jnp.broadcast_to(mix[:1].astype(F32), (HALO, LANES))
    last = jnp.broadcast_to(mix[tokens - 1 :].astype(F32), (HALO, LANES))
    message_ref[half + share :, :] = jnp.where(row == 0, first, last).astype(BF16)


def project_second(natural, *refs):
    scaled_ref, inv_ref, query_w_ref, gate_w_ref, cos_ref, sin_ref, mix_ref, taps_ref = refs[:8]
    halos, (keep_ref, send_ref, both_ref) = refs[8:-3], refs[-3:]
    scaled = scaled_ref[...]
    inv = inv_ref[...]
    scale = (NOPE + ROPE) ** (-0.5)
    query = dot_nt(scaled, query_w_ref[...])
    both_ref[:, :NOPE] = query[:, :NOPE] * inv * scale
    both_ref[:, NOPE : NOPE + LANES] = rotate(query[:, NOPE:] * inv, cos_ref[...], sin_ref[...]) * scale

    gate = jnp.dot(scaled, gate_w_ref[...], preferred_element_type=F32) * inv
    mix = mix_ref[...].astype(F32)
    tokens = mix.shape[0]
    place, places = lax.axis_index("sp"), lax.axis_size("sp")

    def edge_of(other, at):
        inside = (other >= 0) & (other < places)
        other = jnp.clip(other, 0, places - 1)
        if natural:
            edges = halos[0][other].astype(F32)
        else:
            edges = jnp.zeros((HALO, LANES), F32)
            for i, ref in enumerate(halos):
                edges = jnp.where((other ^ place) == i, ref[ref.shape[0] - HALO :, :].astype(F32), edges)
        return jnp.where(inside, edges[at : at + 1, :], 0.0)

    row = lax.broadcasted_iota(jnp.int32, mix.shape, 0)
    earlier = jnp.where(row == 0, edge_of(place - 1, 1), pltpu.roll(mix, 1, 0))
    later = jnp.where(row == tokens - 1, edge_of(place + 1, 0), pltpu.roll(mix, tokens - 1, 0))
    taps = taps_ref[...].astype(F32)
    convolved = taps[0:1] * earlier + taps[1:2] * mix + taps[2:3] * later
    both_ref[:, NOPE + LANES :] = gate * convolved
    core = lax.axis_index("tp") % 2
    rows = tokens // lax.axis_size("tp")
    for i in range(lax.axis_size("tp") // 2):
        for ref, side in ((keep_ref, core), (send_ref, 1 - core)):
            source = pl.ds(pl.multiple_of((2 * i + side) * rows, rows), rows)
            ref[i * rows : (i + 1) * rows, :] = both_ref[source, :].astype(BF16)


def attend(slots, chunk, last, *refs):
    inputs = 1 + max(place for chip_slots in slots for place, _ in chip_slots)
    pieces, refs = refs[:inputs], refs[inputs:]
    gain_ref, expand_refs, query_refs = refs[0], refs[1:3], refs[3:5]
    refs = refs[5:]
    if last:
        stats_in, out_in, own_w_ref, other_w_ref = refs[:4]
        block_refs, (keep_log_ref, send_log_ref, both_ref) = refs[4:-5], refs[-5:-2]
    else:
        stats_ref, out_ref = refs[:2]
    latent_ref, rope_ref = refs[-2:]
    rank = lax.axis_index("tp")
    chip = rank // 2
    pairs = len(slots)
    half = query_refs[0].shape[0]
    tokens = 2 * half
    group = half // 2
    share = group // pairs
    entries = pairs * LANES

    low = low_lanes((half, LANES))
    queries = []
    for ref in query_refs:
        nope, rope = ref[:, :NOPE], ref[:, NOPE : NOPE + LANES]
        zeros = jnp.zeros_like(rope)
        sides = (jnp.where(low, rope, zeros), jnp.where(low, zeros, rope))
        queries.append([jnp.concatenate([nope, side], axis=1) for side in sides])
    key_w = jnp.concatenate([ref[:, :NOPE] for ref in expand_refs], axis=1)
    value_w = jnp.concatenate([ref[:, NOPE:] for ref in expand_refs], axis=1)
    views = [(chip ^ i, chip_slots) for i, chip_slots in enumerate(slots)]

    def rows_of(chip_slots, slot, first, start, count):
        place, at = chip_slots[slot if first is None else 0]
        at = at if first is None else first + slot
        rows = slice(start, start + count)
        return pieces[place][rows, :] if at is None else pieces[place][at, rows, :]

    def one_chunk(first, state):
        for slot in range(chunk):
            total = jnp.zeros((half, LANES), F32)
            for owner, chip_slots in views:
                piece = rows_of(chip_slots, slot, first, 0, half).astype(F32)
                total = total + piece * piece
                start = pl.multiple_of(slot * group + owner * share, share)
                rope_ref[pl.ds(start, share), :] = rows_of(chip_slots, slot, first, half, share)
            inv = lax.rsqrt(jnp.sum(total, axis=1, keepdims=True) / entries + EPSILON)
            for owner, chip_slots in views:
                piece = rows_of(chip_slots, slot, first, 0, half).astype(F32)
                columns = pl.ds(pl.multiple_of(owner * LANES, LANES), LANES)
                scaled = (piece * inv * gain_ref[:, columns]).astype(BF16)
                for side in range(2):
                    base = (side * chunk + slot) * group
                    latent_ref[base : base + group, columns] = scaled[side * group : (side + 1) * group]
        latent = latent_ref[...]
        keys = jnp.dot(latent, key_w, preferred_element_type=F32).astype(BF16)
        values = lax.dot_general(
            value_w, latent, (((0,), (1,)), ((), ())), preferred_element_type=F32
        ).astype(BF16)
        rope = rope_ref[...]
        count = chunk * group
        spans = [slice(i * count, (i + 1) * count) for i in range(2)]
        heads = [slice(i * NOPE, (i + 1) * NOPE) for i in range(2)]
        scores = [
            jnp.concatenate(
                [dot_nt(jnp.concatenate([keys[span, head], rope], axis=1), query[i]) for head, query in zip(heads, queries)],
                axis=1,
            )
            for i, span in enumerate(spans)
        ]
        peak = jnp.max(jnp.maximum(*scores), axis=0, keepdims=True)
        if state is not None:
            peak = jnp.maximum(peak, state[0])
        weights = [jnp.exp(piece - peak) for piece in scores]
        total = jnp.sum(weights[0] + weights[1], axis=0, keepdims=True)
        weights = [piece.astype(BF16) for piece in weights]
        out = jnp.concatenate(
            [
                sum(
                    jnp.dot(values[head, span], weight[:, i * half : (i + 1) * half], preferred_element_type=F32)
                    for span, weight in zip(spans, weights)
                )
                for i, head in enumerate(heads)
            ],
            axis=1,
        )
        if state is not None:
            rescale = jnp.exp(state[0] - peak)
            total = total + state[1] * rescale
            out = out + state[2] * rescale
        return peak, total, out

    state = (stats_in[0:1], stats_in[1:2], out_in[...]) if last else None
    if chunk == len(views[0][1]):
        peak, total, out = one_chunk(None, state)
    else:
        if state is None:
            state = (
                jnp.full((1, tokens), -jnp.inf, F32),
                jnp.zeros((1, tokens), F32),
                jnp.zeros((VDIM, tokens), F32),
            )
        steps = len(views[0][1]) // chunk
        peak, total, out = lax.fori_loop(0, steps, lambda i, state: one_chunk(i * chunk, state), state)
    if not last:
        stats_ref[0:1] = peak
        stats_ref[1:2] = total
        out_ref[...] = out
        return
    logs = peak + jnp.log(total)
    keep_log_ref[...] = logs[:, :half]
    send_log_ref[...] = logs[:, half:]
    out = out * (1.0 / total)
    rows = half // pairs
    result = None
    for i, weight_ref in enumerate((own_w_ref, other_w_ref)):
        attended = jnp.transpose(out[:, i * half : (i + 1) * half]).astype(BF16)
        both_ref[i, :, :VDIM] = attended
        both_ref[i, :, VDIM:] = query_refs[i][:, NOPE + LANES :]
        order = [both_ref[i, pl.ds(pl.multiple_of((chip ^ j) * rows, rows), rows), :] for j in range(pairs)]
        product = jnp.dot(jnp.concatenate(order, axis=0), weight_ref[...], preferred_element_type=F32)
        result = product if result is None else result + product
    for i, ref in enumerate(block_refs):
        ref[...] = result[i * rows : (i + 1) * rows].astype(ref.dtype)


def join_logs(own_ref, got_ref, log_ref):
    ranks = lax.axis_size("tp")
    rows = log_ref.shape[1] // ranks
    first = lax.axis_index("tp") % 2 == 0
    own, got = own_ref[...], got_ref[...]
    sides = [jnp.where(first, own, got), jnp.where(first, got, own)]
    lane = lax.broadcasted_iota(jnp.int32, log_ref.shape, 1) // rows
    logs = jnp.zeros(log_ref.shape, F32)
    for i in range(ranks):
        side = jnp.concatenate([sides[i % 2]] * 2, axis=1)
        shift = (i - i // 2) * rows
        logs = jnp.where(lane == i, pltpu.roll(side, shift, 1) if shift else side, logs)
    log_ref[...] = logs


def body(
    activations,
    norm_gain,
    query_weight,
    latent_weight,
    rope_key_weight,
    latent_gain,
    expand_weight,
    gate_weight,
    pre_weight,
    value_weight,
    conv_kernel,
    output_attend,
    output_conv,
):
    ranks = lax.axis_size("tp")
    places = lax.axis_size("sp")
    pairs = ranks // 2
    tokens, width = activations.shape
    features = ranks * width
    half = tokens // 2
    share = half // ranks
    rows = tokens // ranks
    channels = gate_weight.shape[1]

    even = [activations] + exchange(activations, "tp", 2, pairs)
    odd = swap_each(even)

    latent_t = latent_weight.T
    partner_t = swap(latent_t, "tp", 1)
    other_expand = swap(expand_weight, "tp", 1)
    key_w, query_w, mix_w, own_w, cosines, sines = kernel_call(
        prepare,
        [
            ((4 * ROPE, features), BF16),
            ((NOPE + 2 * ROPE, features), BF16),
            ((features, 2 * LANES), BF16),
            ((VDIM + channels, features), BF16),
            ((tokens, LANES), F32),
            ((tokens, LANES), F32),
        ],
        16 << 20,
        scratch=[pltpu.SemaphoreType.DMA((9,))],
        flops=1 << 28,
        nbytes=1 << 23,
        in_hbm=range(7),
    )(
        latent_t, rope_key_weight.T, query_weight.T, pre_weight, value_weight, output_attend, output_conv,
        partner_t,
    )
    other_w = swap(own_w, "tp", 1)

    scaled, inv, message, mix = kernel_call(
        functools.partial(project_first, pairs),
        [
            ((tokens, features), BF16),
            ((tokens, LANES), F32),
            ((half + share + HALO, LANES), BF16),
            ((tokens, channels), BF16),
        ],
        12 << 20,
        scratch=[pltpu.VMEM((tokens, 2 * LANES), F32)],
        flops=2 * tokens * features * 4 * LANES,
        nbytes=4 * tokens * features,
    )(*even, *odd, norm_gain.reshape(1, -1), key_w, mix_w, cosines, sines)

    small = places <= 8 and places & (places - 1) == 0
    if small:
        halos = [message] + exchange(message, "sp", 1, places)
        near = message[: half + share]
        nears = [near] + exchange(near, "tp", 2, pairs)
        near_other = swap(jnp.stack(nears), "tp", 1)
        around = jnp.stack([piece[: half + share] for piece in halos[1:]])
    else:
        around = lax.all_gather(message, "sp", axis=0)
        around, halos = around[:, : half + share], [around[:, half + share :]]
    arounds = [around] + exchange(around, "tp", 2, pairs)
    others = swap_each(arounds)
    blocks = range(places - 1) if small else range(places)
    slots = [[(i, k) for k in blocks] for i in range(pairs)]
    other_slots = slots
    if small:
        other_slots = [[(pairs, i)] + chip_slots for i, chip_slots in enumerate(slots)]
        slots = [[(pairs + i, None)] + chip_slots for i, chip_slots in enumerate(slots)]
        arounds += nears
        others.append(near_other)

    columns = NOPE + LANES + channels
    keep, send = kernel_call(
        functools.partial(project_second, not small),
        [((half, columns), BF16)] * 2,
        12 << 20,
        scratch=[pltpu.VMEM((tokens, columns), F32)],
        flops=2 * tokens * features * 3 * LANES,
        nbytes=4 * tokens * features,
    )(scaled, inv, query_w, gate_weight, cosines, sines, mix, conv_kernel, *halos)
    got = swap(send, "tp", 1)

    chunk = places if small else 4

    def attend_to(arrays, slots, last, outs, *operands):
        scratch = [
            pltpu.VMEM((2, half, VDIM + channels), BF16),
            pltpu.VMEM((chunk * half, pairs * LANES), BF16),
            pltpu.VMEM((chunk * half // 2, LANES), BF16),
        ]
        return kernel_call(
            functools.partial(attend, slots, chunk, last),
            outs,
            (14 << 20) if small else (40 << 20),
            scratch=scratch if last else scratch[1:],
            flops=1 << 29,
            nbytes=1 << 22,
        )(*arrays, latent_gain.reshape(1, -1), expand_weight, other_expand, keep, got, *operands)

    stats, out = attend_to(arounds, slots, False, [((8, tokens), F32), ((VDIM, tokens), F32)])
    *outs, own_log, send_log = attend_to(
        others,
        other_slots,
        True,
        [((rows, features), F32)] + [((rows, features), BF16)] * (pairs - 1) + [((1, half), F32)] * 2,
        stats,
        out,
        own_w,
        other_w,
    )
    arrived = exchange_blocks(outs)
    got_log = swap(send_log, "tp", 1)
    (logs,) = kernel_call(join_logs, [((1, tokens), F32)], 1 << 20, flops=1 << 22, nbytes=1 << 12)(own_log, got_log)
    total = outs[0]
    for piece in arrived:
        total = total + piece.astype(F32)
    return total.astype(BF16), logs


def solution(mesh):
    return jax.shard_map(
        body,
        mesh=mesh,
        in_specs=(
            P("sp", "tp"),
            P(),
            P(None, "tp"),
            P(None, "tp"),
            P(),
            P(),
            P(None, "tp"),
            P(None, "tp"),
            P(None, "tp"),
            P(None, "tp"),
            P(None, "tp"),
            P("tp", None),
            P("tp", None),
        ),
        out_specs=(P(("sp", "tp"), None), P("tp", "sp")),
        check_vma=False,
    )
```

```python
import functools
import math

import jax
import jax.numpy as jnp
from jax import lax
from jax.experimental import pallas as pl
from jax.experimental.pallas import tpu as pltpu
from jax.sharding import PartitionSpec as P


NOPE = 128
ROPE = 64
VDIM = 128
GRID_W = 64
EPSILON = 1e-06
ROPE_BASE = 10000.0
LANES = 128
HALO = 8
F32 = jnp.float32
BF16 = jnp.bfloat16


def swap(array, axis, mask):
    peers = lax.axis_size(axis)
    return lax.ppermute(array, axis, [(i, i ^ mask) for i in range(peers)])


def exchange(array, axis, stride, peers):
    pieces = []
    for i in reversed(range(1, peers)):
        pieces.append(swap(array, axis, stride * i))
    return pieces[::-1]


def swap_each(arrays):
    pieces = []
    for array in arrays:
        pieces.append(swap(array, "tp", 1))
    return pieces


def exchange_blocks(blocks):
    arrived = []
    for i in reversed(range(1, len(blocks))):
        arrived.append(swap(blocks[i], "tp", 2 * i))
    return arrived


def kernel_call(body, outs, limit, scratch=(), flops=0, nbytes=0, in_hbm=()):
    whole = pl.BlockSpec(memory_space=pltpu.VMEM)

    def call(*operands):
        spaces = [pltpu.HBM if i in in_hbm else pltpu.VMEM for i in range(len(operands))]
        operands = [
            pltpu.with_memory_space_constraint(operand, space) if space is pltpu.HBM else operand
            for operand, space in zip(operands, spaces, strict=True)
        ]
        return pl.pallas_call(
            body,
            out_shape=[jax.ShapeDtypeStruct(shape, dtype) for shape, dtype in outs],
            in_specs=[pl.BlockSpec(memory_space=space) for space in spaces],
            out_specs=[whole] * len(outs),
            scratch_shapes=list(scratch),
            compiler_params=pltpu.CompilerParams(vmem_limit_bytes=limit),
            cost_estimate=pl.CostEstimate(flops=flops, bytes_accessed=nbytes, transcendentals=0),
        )(*operands)

    return call


def rotate(values, cosines, sines):
    quarter = ROPE // 4
    lane = lax.broadcasted_iota(jnp.int32, values.shape, 1)
    first = (lane // quarter) % 2 == 0
    ahead = pltpu.roll(values, LANES - quarter, 1)
    behind = pltpu.roll(values, quarter, 1)
    return values * cosines + jnp.where(first, ahead, behind) * sines


def low_lanes(shape):
    return lax.broadcasted_iota(jnp.int32, shape, 1) < ROPE


def prepare(
    latent_ref, rope_ref, query_ref, pre_ref, value_ref, attend_ref, conv_ref, expand_ref, partner_ref,
    key_w_ref, query_w_ref, mix_w_ref, own_w_ref, cos_ref, sin_ref, sems,
):
    core = lax.axis_index("tp") % 2
    mine = pl.ds(pl.multiple_of(core * ROPE, ROPE), ROPE)
    moves = [
        (latent_ref, key_w_ref.at[mine]),
        (rope_ref, key_w_ref.at[2 * ROPE : 3 * ROPE]),
        (rope_ref, key_w_ref.at[3 * ROPE :]),
        (pre_ref, mix_w_ref.at[:, :LANES]),
        (value_ref, mix_w_ref.at[:, LANES:]),
        (query_ref, query_w_ref.at[: NOPE + ROPE]),
        (query_ref.at[NOPE:], query_w_ref.at[NOPE + ROPE :]),
        (attend_ref, own_w_ref.at[:VDIM]),
        (conv_ref, own_w_ref.at[VDIM : 2 * VDIM]),
    ]
    wide = NOPE + VDIM
    high = own_w_ref.shape[0] - 2 * VDIM
    for k in range(own_w_ref.shape[1] // wide):
        target = own_w_ref.at[2 * VDIM :, k * wide : (k + 1) * wide]
        moves.append((expand_ref.at[k * high : (k + 1) * high], target))
    copies = [pltpu.make_async_copy(source, target, sems.at[i]) for i, (source, target) in enumerate(moves)]
    for copy in copies:
        copy.start()
    key_w_ref[pl.ds(pl.multiple_of((1 - core) * ROPE, ROPE), ROPE), :] = partner_ref[...]
    quarter = ROPE // 4
    groups = cos_ref.shape[0] // GRID_W
    first_row = lax.axis_index("sp") * groups

    def angles(rows, start):
        lane = lax.broadcasted_iota(jnp.int32, (rows, LANES), 1) % ROPE
        place = (lax.broadcasted_iota(jnp.int32, (rows, LANES), 0) + start).astype(F32)
        inverse = jnp.exp((lane % quarter).astype(F32) * (-math.log(ROPE_BASE) / quarter))
        angle = place * inverse
        sign = jnp.where((lane // quarter) % 2 == 0, -1.0, 1.0)
        return lane < 2 * quarter, jnp.cos(angle), jnp.sin(angle) * sign

    _, row_cos, row_sin = angles(groups, first_row)
    by_row, col_cos, col_sin = angles(GRID_W, 0)
    for g in range(groups):
        rows = slice(g * GRID_W, (g + 1) * GRID_W)
        cos_ref[rows, :] = jnp.where(by_row, row_cos[g : g + 1], col_cos)
        sin_ref[rows, :] = jnp.where(by_row, row_sin[g : g + 1], col_sin)
    for copy in copies:
        copy.wait()


def dot_nt(left, right):
    return lax.dot_general(left, right, (((1,), (1,)), ((), ())), preferred_element_type=F32)


def project_first(pairs, *refs):
    pieces, refs = refs[: 2 * pairs], refs[2 * pairs :]
    gain_ref, key_w_ref, mix_w_ref, cos_ref, sin_ref = refs[:5]
    scaled_ref, inv_ref, message_ref, mix_ref, key_ref = refs[5:]
    rank = lax.axis_index("tp")
    tokens, width = pieces[0].shape
    half = tokens // 2
    total = jnp.zeros((tokens, LANES), F32)
    for i, ref in enumerate(pieces):
        owner = rank ^ (2 * (i % pairs) + i // pairs)
        piece = ref[...].astype(F32)
        squares = piece * piece
        for j in range(width // LANES):
            total = total + squares[:, j * LANES : (j + 1) * LANES]
        columns = pl.ds(pl.multiple_of(owner * width, width), width)
        scaled_ref[:, columns] = (piece * gain_ref[:, columns]).astype(BF16)
    features = 2 * pairs * width
    inv = lax.rsqrt(jnp.sum(total, axis=1, keepdims=True) / features + EPSILON)
    inv_ref[...] = jnp.broadcast_to(inv, inv_ref.shape)
    scaled = scaled_ref[...]
    keys = dot_nt(scaled, key_w_ref[...]) * inv
    mixes = jnp.dot(scaled, mix_w_ref[...], preferred_element_type=F32) * inv
    mix = (mixes[:, :LANES] * mixes[:, LANES:]).astype(BF16)
    mix_ref[...] = mix
    key_ref[...] = keys
    chip, core = rank // 2, rank % 2
    start = pl.multiple_of(core * half, half)
    message_ref[:half, :] = key_ref[pl.ds(start, half), :LANES].astype(BF16)
    share = half // (2 * pairs)
    turned = []
    for base in (0, half // 2):
        rows = pl.ds(pl.multiple_of(start + base + chip * share, share), share)
        turned.append(rotate(key_ref[rows, LANES:], cos_ref[rows, :], sin_ref[rows, :]))
    low = low_lanes((share, LANES))
    message_ref[half : half + share, :] = jnp.where(low, turned[0], turned[1]).astype(BF16)
    row = lax.broadcasted_iota(jnp.int32, (HALO, LANES), 0)
    first = jnp.broadcast_to(mix[:1].astype(F32), (HALO, LANES))
    last = jnp.broadcast_to(mix[tokens - 1 :].astype(F32), (HALO, LANES))
    message_ref[half + share :, :] = jnp.where(row == 0, first, last).astype(BF16)


def project_second(natural, *refs):
    scaled_ref, inv_ref, query_w_ref, gate_w_ref, cos_ref, sin_ref, mix_ref, taps_ref = refs[:8]
    halos, (keep_ref, send_ref, both_ref) = refs[8:-3], refs[-3:]
    scaled = scaled_ref[...]
    inv = inv_ref[...]
    scale = (NOPE + ROPE) ** (-0.5)
    query = dot_nt(scaled, query_w_ref[...])
    both_ref[:, :NOPE] = query[:, :NOPE] * inv * scale
    both_ref[:, NOPE : NOPE + LANES] = rotate(query[:, NOPE:] * inv, cos_ref[...], sin_ref[...]) * scale

    gate = jnp.dot(scaled, gate_w_ref[...], preferred_element_type=F32) * inv
    mix = mix_ref[...].astype(F32)
    tokens = mix.shape[0]
    place, places = lax.axis_index("sp"), lax.axis_size("sp")

    def edge_of(other, at):
        inside = (other >= 0) & (other < places)
        other = jnp.clip(other, 0, places - 1)
        if natural:
            edges = halos[0][other].astype(F32)
        else:
            edges = jnp.zeros((HALO, LANES), F32)
            for i, ref in enumerate(halos):
                edges = jnp.where((other ^ place) == i, ref[ref.shape[0] - HALO :, :].astype(F32), edges)
        return jnp.where(inside, edges[at : at + 1, :], 0.0)

    row = lax.broadcasted_iota(jnp.int32, mix.shape, 0)
    earlier = jnp.where(row == 0, edge_of(place - 1, 1), pltpu.roll(mix, 1, 0))
    later = jnp.where(row == tokens - 1, edge_of(place + 1, 0), pltpu.roll(mix, tokens - 1, 0))
    taps = taps_ref[...].astype(F32)
    convolved = taps[0:1] * earlier + taps[1:2] * mix + taps[2:3] * later
    both_ref[:, NOPE + LANES :] = gate * convolved
    core = lax.axis_index("tp") % 2
    rows = tokens // lax.axis_size("tp")
    for i in range(lax.axis_size("tp") // 2):
        for ref, side in ((keep_ref, core), (send_ref, 1 - core)):
            source = pl.ds(pl.multiple_of((2 * i + side) * rows, rows), rows)
            ref[i * rows : (i + 1) * rows, :] = both_ref[source, :].astype(BF16)


def attend(slots, chunk, stage, *refs):
    inputs = 1 + max(place for chip_slots in slots for place, _ in chip_slots)
    pieces, refs = refs[:inputs], refs[inputs:]
    gain_ref, own_w_ref, other_w_ref, query_refs = refs[0], refs[1], refs[2], refs[3:5]
    refs = refs[5:]
    if stage > 0:
        stats_in, out_in = refs[:2]
        refs = refs[2:]
    last = stage == 2
    if last:
        block_refs, (keep_log_ref, send_log_ref, both_ref) = refs[:-5], refs[-5:-2]
    else:
        stats_ref, out_ref = refs[:2]
    latent_ref, rope_ref = refs[-2:]
    rank = lax.axis_index("tp")
    chip = rank // 2
    pairs = len(slots)
    half = query_refs[0].shape[0]
    tokens = 2 * half
    group = half // 2
    share = group // pairs
    entries = pairs * LANES

    low = low_lanes((half, LANES))
    queries = []
    for ref in query_refs:
        nope, rope = ref[:, :NOPE], ref[:, NOPE : NOPE + LANES]
        zeros = jnp.zeros_like(rope)
        sides = (jnp.where(low, rope, zeros), jnp.where(low, zeros, rope))
        queries.append([jnp.concatenate([nope, side], axis=1) for side in sides])
    wide = NOPE + VDIM
    starts = range(0, own_w_ref.shape[1], wide)

    def expansion(ref, begin, size):
        return jnp.concatenate([ref[2 * VDIM :, k + begin : k + begin + size] for k in starts], axis=0)

    key_w = jnp.concatenate([expansion(ref, 0, NOPE) for ref in (own_w_ref, other_w_ref)], axis=1)
    value_w = jnp.concatenate([expansion(ref, NOPE, VDIM) for ref in (own_w_ref, other_w_ref)], axis=1)
    views = [(chip ^ i, chip_slots) for i, chip_slots in enumerate(slots)]

    def rows_of(chip_slots, slot, first, start, count):
        place, at = chip_slots[slot if first is None else 0]
        at = at if first is None else first + slot
        rows = slice(start, start + count)
        return pieces[place][rows, :] if at is None else pieces[place][at, rows, :]

    def one_chunk(first, state):
        for slot in range(chunk):
            total = jnp.zeros((half, LANES), F32)
            for owner, chip_slots in views:
                piece = rows_of(chip_slots, slot, first, 0, half).astype(F32)
                total = total + piece * piece
                start = pl.multiple_of(slot * group + owner * share, share)
                rope_ref[pl.ds(start, share), :] = rows_of(chip_slots, slot, first, half, share)
            inv = lax.rsqrt(jnp.sum(total, axis=1, keepdims=True) / entries + EPSILON)
            for owner, chip_slots in views:
                piece = rows_of(chip_slots, slot, first, 0, half).astype(F32)
                columns = pl.ds(pl.multiple_of(owner * LANES, LANES), LANES)
                scaled = (piece * inv * gain_ref[:, columns]).astype(BF16)
                for side in range(2):
                    base = (side * chunk + slot) * group
                    latent_ref[base : base + group, columns] = scaled[side * group : (side + 1) * group]
        latent = latent_ref[...]
        keys = jnp.dot(latent, key_w, preferred_element_type=F32).astype(BF16)
        values = lax.dot_general(
            value_w, latent, (((0,), (1,)), ((), ())), preferred_element_type=F32
        ).astype(BF16)
        rope = rope_ref[...]
        count = chunk * group
        spans = [slice(i * count, (i + 1) * count) for i in range(2)]
        heads = [slice(i * NOPE, (i + 1) * NOPE) for i in range(2)]
        scores = [
            jnp.concatenate(
                [dot_nt(jnp.concatenate([keys[span, head], rope], axis=1), query[i]) for head, query in zip(heads, queries)],
                axis=1,
            )
            for i, span in enumerate(spans)
        ]
        peak = jnp.max(jnp.maximum(*scores), axis=0, keepdims=True)
        if state is not None:
            peak = jnp.maximum(peak, state[0])
        weights = [jnp.exp(piece - peak) for piece in scores]
        total = jnp.sum(weights[0] + weights[1], axis=0, keepdims=True)
        weights = [piece.astype(BF16) for piece in weights]
        out = jnp.concatenate(
            [
                sum(
                    jnp.dot(values[head, span], weight[:, i * half : (i + 1) * half], preferred_element_type=F32)
                    for span, weight in zip(spans, weights)
                )
                for i, head in enumerate(heads)
            ],
            axis=1,
        )
        if state is not None:
            rescale = jnp.exp(state[0] - peak)
            total = total + state[1] * rescale
            out = out + state[2] * rescale
        return peak, total, out

    state = (stats_in[0:1], stats_in[1:2], out_in[...]) if stage > 0 else None
    if chunk == len(views[0][1]):
        peak, total, out = one_chunk(None, state)
    else:
        if state is None:
            state = (
                jnp.full((1, tokens), -jnp.inf, F32),
                jnp.zeros((1, tokens), F32),
                jnp.zeros((VDIM, tokens), F32),
            )
        steps = len(views[0][1]) // chunk
        peak, total, out = lax.fori_loop(0, steps, lambda i, state: one_chunk(i * chunk, state), state)
    if not last:
        stats_ref[0:1] = peak
        stats_ref[1:2] = total
        out_ref[...] = out
        return
    logs = peak + jnp.log(total)
    keep_log_ref[...] = logs[:, :half]
    send_log_ref[...] = logs[:, half:]
    out = out * (1.0 / total)
    rows = half // pairs
    result = None
    for i, weight_ref in enumerate((own_w_ref, other_w_ref)):
        attended = jnp.transpose(out[:, i * half : (i + 1) * half]).astype(BF16)
        both_ref[i, :, :VDIM] = attended
        both_ref[i, :, VDIM:] = query_refs[i][:, NOPE + LANES :]
        order = [both_ref[i, pl.ds(pl.multiple_of((chip ^ j) * rows, rows), rows), :] for j in range(pairs)]
        product = jnp.dot(jnp.concatenate(order, axis=0), weight_ref[: 2 * VDIM], preferred_element_type=F32)
        result = product if result is None else result + product
    for i, ref in enumerate(block_refs):
        ref[...] = result[i * rows : (i + 1) * rows].astype(ref.dtype)


def join_logs(own_ref, got_ref, log_ref):
    ranks = lax.axis_size("tp")
    rows = log_ref.shape[1] // ranks
    first = lax.axis_index("tp") % 2 == 0
    own, got = own_ref[...], got_ref[...]
    sides = [jnp.where(first, own, got), jnp.where(first, got, own)]
    lane = lax.broadcasted_iota(jnp.int32, log_ref.shape, 1) // rows
    logs = jnp.zeros(log_ref.shape, F32)
    for i in range(ranks):
        side = jnp.concatenate([sides[i % 2]] * 2, axis=1)
        shift = (i - i // 2) * rows
        logs = jnp.where(lane == i, pltpu.roll(side, shift, 1) if shift else side, logs)
    log_ref[...] = logs


def body(
    activations,
    norm_gain,
    query_weight,
    latent_weight,
    rope_key_weight,
    latent_gain,
    expand_weight,
    gate_weight,
    pre_weight,
    value_weight,
    conv_kernel,
    output_attend,
    output_conv,
):
    ranks = lax.axis_size("tp")
    places = lax.axis_size("sp")
    pairs = ranks // 2
    tokens, width = activations.shape
    features = ranks * width
    half = tokens // 2
    share = half // ranks
    rows = tokens // ranks
    channels = gate_weight.shape[1]

    even = [activations] + exchange(activations, "tp", 2, pairs)
    odd = swap_each(even)

    latent_t = latent_weight.T
    partner_t = swap(latent_t, "tp", 1)
    key_w, query_w, mix_w, own_w, cosines, sines = kernel_call(
        prepare,
        [
            ((4 * ROPE, features), BF16),
            ((NOPE + 2 * ROPE, features), BF16),
            ((features, 2 * LANES), BF16),
            ((VDIM + channels + expand_weight.size // features, features), BF16),
            ((tokens, LANES), F32),
            ((tokens, LANES), F32),
        ],
        16 << 20,
        scratch=[pltpu.SemaphoreType.DMA((9 + features // (NOPE + VDIM),))],
        flops=1 << 28,
        nbytes=1 << 23,
        in_hbm=range(8),
    )(
        latent_t, rope_key_weight.T, query_weight.T, pre_weight, value_weight, output_attend, output_conv,
        expand_weight, partner_t,
    )
    other_w = swap(own_w, "tp", 1)

    scaled, inv, message, mix = kernel_call(
        functools.partial(project_first, pairs),
        [
            ((tokens, features), BF16),
            ((tokens, LANES), F32),
            ((half + share + HALO, LANES), BF16),
            ((tokens, channels), BF16),
        ],
        12 << 20,
        scratch=[pltpu.VMEM((tokens, 2 * LANES), F32)],
        flops=2 * tokens * features * 4 * LANES,
        nbytes=4 * tokens * features,
    )(*even, *odd, norm_gain.reshape(1, -1), key_w, mix_w, cosines, sines)

    small = places <= 8 and places & (places - 1) == 0
    if small:
        halos = [message] + exchange(message, "sp", 1, places)
        near = message[: half + share]
        nears = [near] + exchange(near, "tp", 2, pairs)
        near_other = swap(jnp.stack(nears), "tp", 1)
        around = jnp.stack([piece[: half + share] for piece in halos[1:]])
    else:
        around = lax.all_gather(message, "sp", axis=0)
        around, halos = around[:, : half + share], [around[:, half + share :]]
    arounds = [around] + exchange(around, "tp", 2, pairs)
    others = swap_each(arounds)
    slots = [[(i, k) for k in (range(places - 1) if small else range(places))] for i in range(pairs)]

    columns = NOPE + LANES + channels
    keep, send = kernel_call(
        functools.partial(project_second, not small),
        [((half, columns), BF16)] * 2,
        12 << 20,
        scratch=[pltpu.VMEM((tokens, columns), F32)],
        flops=2 * tokens * features * 3 * LANES,
        nbytes=4 * tokens * features,
    )(scaled, inv, query_w, gate_weight, cosines, sines, mix, conv_kernel, *halos)
    got = swap(send, "tp", 1)

    def attend_to(arrays, slots, stage, outs, *state):
        chunk = len(slots[0]) if small else 4
        scratch = [
            pltpu.VMEM((2, half, VDIM + channels), BF16),
            pltpu.VMEM((chunk * half, pairs * LANES), BF16),
            pltpu.VMEM((chunk * half // 2, LANES), BF16),
        ]
        return kernel_call(
            functools.partial(attend, slots, chunk, stage),
            outs,
            (14 << 20) if small else (40 << 20),
            scratch=scratch if stage == 2 else scratch[1:],
            flops=1 << 29,
            nbytes=1 << 22,
        )(*arrays, latent_gain.reshape(1, -1), own_w, other_w, keep, got, *state)

    state_outs = [((8, tokens), F32), ((VDIM, tokens), F32)]
    state = []
    if small:
        near_slots = [[(i, None), (pairs, i)] for i in range(pairs)]
        state = attend_to([*nears, near_other], near_slots, 0, state_outs)
    state = attend_to(arounds, slots, 1 if small else 0, state_outs, *state)
    final_outs = [((rows, features), F32)] + [((rows, features), BF16)] * (pairs - 1) + [((1, half), F32)] * 2
    *outs, own_log, send_log = attend_to(others, slots, 2, final_outs, *state)
    arrived = exchange_blocks(outs)
    got_log = swap(send_log, "tp", 1)
    (logs,) = kernel_call(join_logs, [((1, tokens), F32)], 1 << 20, flops=1 << 22, nbytes=1 << 12)(own_log, got_log)
    total = outs[0]
    for piece in arrived:
        total = total + piece.astype(F32)
    return total.astype(BF16), logs


def solution(mesh):
    return jax.shard_map(
        body,
        mesh=mesh,
        in_specs=(
            P("sp", "tp"),
            P(),
            P(None, "tp"),
            P(None, "tp"),
            P(),
            P(),
            P(None, "tp"),
            P(None, "tp"),
            P(None, "tp"),
            P(None, "tp"),
            P(None, "tp"),
            P("tp", None),
            P("tp", None),
        ),
        out_specs=(P(("sp", "tp"), None), P("tp", "sp")),
        check_vma=False,
    )
```

```python
import functools
import math

import jax
import jax.numpy as jnp
from jax import lax
from jax.experimental import pallas as pl
from jax.experimental.pallas import tpu as pltpu
from jax.sharding import PartitionSpec as P


NOPE = 128
ROPE = 64
VDIM = 128
GRID_W = 64
EPSILON = 1e-06
ROPE_BASE = 10000.0
LANES = 128
HALO = 8
F32 = jnp.float32
BF16 = jnp.bfloat16


def swap(array, axis, mask):
    peers = lax.axis_size(axis)
    return lax.ppermute(array, axis, [(i, i ^ mask) for i in range(peers)])


def exchange(array, axis, stride, peers):
    pieces = []
    for i in reversed(range(1, peers)):
        pieces.append(swap(array, axis, stride * i))
    return pieces[::-1]


def swap_each(arrays):
    pieces = []
    for array in arrays:
        pieces.append(swap(array, "tp", 1))
    return pieces


def exchange_blocks(blocks):
    arrived = []
    for i in reversed(range(1, len(blocks))):
        arrived.append(swap(blocks[i], "tp", 2 * i))
    return arrived


def kernel_call(body, outs, limit, scratch=(), flops=0, nbytes=0, in_hbm=()):
    whole = pl.BlockSpec(memory_space=pltpu.VMEM)

    def call(*operands):
        spaces = [pltpu.HBM if i in in_hbm else pltpu.VMEM for i in range(len(operands))]
        operands = [
            pltpu.with_memory_space_constraint(operand, space) if space is pltpu.HBM else operand
            for operand, space in zip(operands, spaces, strict=True)
        ]
        return pl.pallas_call(
            body,
            out_shape=[jax.ShapeDtypeStruct(shape, dtype) for shape, dtype in outs],
            in_specs=[pl.BlockSpec(memory_space=space) for space in spaces],
            out_specs=[whole] * len(outs),
            scratch_shapes=list(scratch),
            compiler_params=pltpu.CompilerParams(vmem_limit_bytes=limit),
            cost_estimate=pl.CostEstimate(flops=flops, bytes_accessed=nbytes, transcendentals=0),
        )(*operands)

    return call


def rotate(values, cosines, sines):
    quarter = ROPE // 4
    lane = lax.broadcasted_iota(jnp.int32, values.shape, 1)
    first = (lane // quarter) % 2 == 0
    ahead = pltpu.roll(values, LANES - quarter, 1)
    behind = pltpu.roll(values, quarter, 1)
    return values * cosines + jnp.where(first, ahead, behind) * sines


def low_lanes(shape):
    return lax.broadcasted_iota(jnp.int32, shape, 1) < ROPE


def prepare(
    latent_ref, rope_ref, query_ref, pre_ref, value_ref, attend_ref, conv_ref, expand_ref, partner_ref,
    key_w_ref, query_w_ref, mix_w_ref, own_w_ref, cos_ref, sin_ref, sems,
):
    core = lax.axis_index("tp") % 2
    mine = pl.ds(pl.multiple_of(core * ROPE, ROPE), ROPE)
    moves = [
        (latent_ref, key_w_ref.at[mine]),
        (rope_ref, key_w_ref.at[2 * ROPE : 3 * ROPE]),
        (rope_ref, key_w_ref.at[3 * ROPE :]),
        (pre_ref, mix_w_ref.at[:, :LANES]),
        (value_ref, mix_w_ref.at[:, LANES:]),
        (query_ref, query_w_ref.at[: NOPE + ROPE]),
        (query_ref.at[NOPE:], query_w_ref.at[NOPE + ROPE :]),
        (attend_ref, own_w_ref.at[:VDIM]),
        (conv_ref, own_w_ref.at[VDIM : 2 * VDIM]),
    ]
    wide = NOPE + VDIM
    high = own_w_ref.shape[0] - 2 * VDIM
    for k in range(own_w_ref.shape[1] // wide):
        target = own_w_ref.at[2 * VDIM :, k * wide : (k + 1) * wide]
        moves.append((expand_ref.at[k * high : (k + 1) * high], target))
    copies = [pltpu.make_async_copy(source, target, sems.at[i]) for i, (source, target) in enumerate(moves)]
    for copy in copies:
        copy.start()
    key_w_ref[pl.ds(pl.multiple_of((1 - core) * ROPE, ROPE), ROPE), :] = partner_ref[...]
    quarter = ROPE // 4
    groups = cos_ref.shape[0] // GRID_W
    first_row = lax.axis_index("sp") * groups

    def angles(rows, start):
        lane = lax.broadcasted_iota(jnp.int32, (rows, LANES), 1) % ROPE
        place = (lax.broadcasted_iota(jnp.int32, (rows, LANES), 0) + start).astype(F32)
        inverse = jnp.exp((lane % quarter).astype(F32) * (-math.log(ROPE_BASE) / quarter))
        angle = place * inverse
        sign = jnp.where((lane // quarter) % 2 == 0, -1.0, 1.0)
        return lane < 2 * quarter, jnp.cos(angle), jnp.sin(angle) * sign

    _, row_cos, row_sin = angles(groups, first_row)
    by_row, col_cos, col_sin = angles(GRID_W, 0)
    for g in range(groups):
        rows = slice(g * GRID_W, (g + 1) * GRID_W)
        cos_ref[rows, :] = jnp.where(by_row, row_cos[g : g + 1], col_cos)
        sin_ref[rows, :] = jnp.where(by_row, row_sin[g : g + 1], col_sin)
    for copy in copies:
        copy.wait()


def dot_nt(left, right):
    return lax.dot_general(left, right, (((1,), (1,)), ((), ())), preferred_element_type=F32)


def weights_for(ref, owners, width, axis):
    spans = [pl.ds(pl.multiple_of(owner * width, width), width) for owner in owners]
    return jnp.concatenate([ref[:, span] if axis else ref[span, :] for span in spans], axis=axis)


def owners_of(core, pairs):
    return [lax.axis_index("tp") ^ (2 * i + core) for i in range(pairs)]


def project(core, pieces, gain_ref, key_w_ref, mix_w_ref, scaled_ref):
    owners = owners_of(core, len(pieces))
    tokens, width = pieces[0].shape
    total = jnp.zeros((tokens, LANES), F32)
    for i, (owner, ref) in enumerate(zip(owners, pieces)):
        piece = ref[...].astype(F32)
        squares = piece * piece
        for j in range(width // LANES):
            total = total + squares[:, j * LANES : (j + 1) * LANES]
        gain = gain_ref[:, pl.ds(pl.multiple_of(owner * width, width), width)]
        scaled_ref[:, i * width : (i + 1) * width] = (piece * gain).astype(BF16)
    scaled = scaled_ref[...]
    keys = dot_nt(scaled, weights_for(key_w_ref, owners, width, 1))
    mixes = jnp.dot(scaled, weights_for(mix_w_ref, owners, width, 0), preferred_element_type=F32)
    return total, keys, mixes


def project_even(pairs, *refs):
    pieces, (gain_ref, key_w_ref, mix_w_ref, scaled_ref, total_ref, keys_ref, mixes_ref) = refs[:pairs], refs[pairs:]
    total, keys, mixes = project(0, pieces, gain_ref, key_w_ref, mix_w_ref, scaled_ref)
    total_ref[...] = total
    keys_ref[...] = keys
    mixes_ref[...] = mixes


def project_first(pairs, *refs):
    pieces, refs = refs[:pairs], refs[pairs:]
    gain_ref, key_w_ref, mix_w_ref, cos_ref, sin_ref, total_ref, keys_ref, mixes_ref = refs[:8]
    scaled_ref, inv_ref, message_ref, mix_ref, key_ref = refs[8:]
    total, keys, mixes = project(1, pieces, gain_ref, key_w_ref, mix_w_ref, scaled_ref)
    rank = lax.axis_index("tp")
    tokens, width = pieces[0].shape
    half = tokens // 2
    features = 2 * pairs * width
    total = jnp.sum(total + total_ref[...], axis=1, keepdims=True)
    inv = lax.rsqrt(total / features + EPSILON)
    inv_ref[...] = jnp.broadcast_to(inv, inv_ref.shape)
    keys = (keys + keys_ref[...]) * inv
    mixes = (mixes + mixes_ref[...]) * inv
    mix = (mixes[:, :LANES] * mixes[:, LANES:]).astype(BF16)
    mix_ref[...] = mix
    key_ref[...] = keys
    chip, core = rank // 2, rank % 2
    start = pl.multiple_of(core * half, half)
    message_ref[:half, :] = key_ref[pl.ds(start, half), :LANES].astype(BF16)
    share = half // (2 * pairs)
    turned = []
    for base in (0, half // 2):
        rows = pl.ds(pl.multiple_of(start + base + chip * share, share), share)
        turned.append(rotate(key_ref[rows, LANES:], cos_ref[rows, :], sin_ref[rows, :]))
    low = low_lanes((share, LANES))
    message_ref[half : half + share, :] = jnp.where(low, turned[0], turned[1]).astype(BF16)
    row = lax.broadcasted_iota(jnp.int32, (HALO, LANES), 0)
    first = jnp.broadcast_to(mix[:1].astype(F32), (HALO, LANES))
    last = jnp.broadcast_to(mix[tokens - 1 :].astype(F32), (HALO, LANES))
    message_ref[half + share :, :] = jnp.where(row == 0, first, last).astype(BF16)


def project_second(natural, *refs):
    even_ref, odd_ref, inv_ref, query_w_ref, gate_w_ref, cos_ref, sin_ref, mix_ref, taps_ref = refs[:9]
    halos, (keep_ref, send_ref, both_ref) = refs[9:-3], refs[-3:]
    pairs = lax.axis_size("tp") // 2
    width = even_ref.shape[1] // pairs
    owners = owners_of(0, pairs) + owners_of(1, pairs)
    scaled = jnp.concatenate([even_ref[...], odd_ref[...]], axis=1)
    inv = inv_ref[...]
    scale = (NOPE + ROPE) ** (-0.5)
    query = dot_nt(scaled, weights_for(query_w_ref, owners, width, 1))
    both_ref[:, :NOPE] = query[:, :NOPE] * inv * scale
    both_ref[:, NOPE : NOPE + LANES] = rotate(query[:, NOPE:] * inv, cos_ref[...], sin_ref[...]) * scale

    gate = jnp.dot(scaled, weights_for(gate_w_ref, owners, width, 0), preferred_element_type=F32) * inv
    mix = mix_ref[...].astype(F32)
    tokens = mix.shape[0]
    place, places = lax.axis_index("sp"), lax.axis_size("sp")

    def edge_of(other, at):
        inside = (other >= 0) & (other < places)
        other = jnp.clip(other, 0, places - 1)
        if natural:
            edges = halos[0][other].astype(F32)
        else:
            edges = jnp.zeros((HALO, LANES), F32)
            for i, ref in enumerate(halos):
                edges = jnp.where((other ^ place) == i, ref[ref.shape[0] - HALO :, :].astype(F32), edges)
        return jnp.where(inside, edges[at : at + 1, :], 0.0)

    row = lax.broadcasted_iota(jnp.int32, mix.shape, 0)
    earlier = jnp.where(row == 0, edge_of(place - 1, 1), pltpu.roll(mix, 1, 0))
    later = jnp.where(row == tokens - 1, edge_of(place + 1, 0), pltpu.roll(mix, tokens - 1, 0))
    taps = taps_ref[...].astype(F32)
    convolved = taps[0:1] * earlier + taps[1:2] * mix + taps[2:3] * later
    both_ref[:, NOPE + LANES :] = gate * convolved
    core = lax.axis_index("tp") % 2
    rows = tokens // lax.axis_size("tp")
    for i in range(lax.axis_size("tp") // 2):
        for ref, side in ((keep_ref, core), (send_ref, 1 - core)):
            source = pl.ds(pl.multiple_of((2 * i + side) * rows, rows), rows)
            ref[i * rows : (i + 1) * rows, :] = both_ref[source, :].astype(BF16)


def attend(slots, chunk, stage, *refs):
    inputs = 1 + max(place for chip_slots in slots for place, _ in chip_slots)
    pieces, refs = refs[:inputs], refs[inputs:]
    gain_ref, own_w_ref, other_w_ref, query_refs = refs[0], refs[1], refs[2], refs[3:5]
    refs = refs[5:]
    if stage > 0:
        stats_in, out_in = refs[:2]
        refs = refs[2:]
    last = stage == 2
    if last:
        block_refs, (keep_log_ref, send_log_ref, both_ref) = refs[:-5], refs[-5:-2]
    else:
        stats_ref, out_ref = refs[:2]
    latent_ref, rope_ref = refs[-2:]
    rank = lax.axis_index("tp")
    chip = rank // 2
    pairs = len(slots)
    half = query_refs[0].shape[0]
    tokens = 2 * half
    group = half // 2
    share = group // pairs
    entries = pairs * LANES

    low = low_lanes((half, LANES))
    queries = []
    for ref in query_refs:
        nope, rope = ref[:, :NOPE], ref[:, NOPE : NOPE + LANES]
        zeros = jnp.zeros_like(rope)
        sides = (jnp.where(low, rope, zeros), jnp.where(low, zeros, rope))
        queries.append([jnp.concatenate([nope, side], axis=1) for side in sides])
    wide = NOPE + VDIM
    starts = range(0, own_w_ref.shape[1], wide)

    def expansion(ref, begin, size):
        return jnp.concatenate([ref[2 * VDIM :, k + begin : k + begin + size] for k in starts], axis=0)

    key_w = jnp.concatenate([expansion(ref, 0, NOPE) for ref in (own_w_ref, other_w_ref)], axis=1)
    value_w = jnp.concatenate([expansion(ref, NOPE, VDIM) for ref in (own_w_ref, other_w_ref)], axis=1)
    views = [(chip ^ i, chip_slots) for i, chip_slots in enumerate(slots)]

    def rows_of(chip_slots, slot, first, start, count):
        place, at = chip_slots[slot if first is None else 0]
        at = at if first is None else first + slot
        rows = slice(start, start + count)
        return pieces[place][rows, :] if at is None else pieces[place][at, rows, :]

    def one_chunk(first, state):
        for slot in range(chunk):
            total = jnp.zeros((half, LANES), F32)
            for owner, chip_slots in views:
                piece = rows_of(chip_slots, slot, first, 0, half).astype(F32)
                total = total + piece * piece
                start = pl.multiple_of(slot * group + owner * share, share)
                rope_ref[pl.ds(start, share), :] = rows_of(chip_slots, slot, first, half, share)
            inv = lax.rsqrt(jnp.sum(total, axis=1, keepdims=True) / entries + EPSILON)
            for owner, chip_slots in views:
                piece = rows_of(chip_slots, slot, first, 0, half).astype(F32)
                columns = pl.ds(pl.multiple_of(owner * LANES, LANES), LANES)
                scaled = (piece * inv * gain_ref[:, columns]).astype(BF16)
                for side in range(2):
                    base = (side * chunk + slot) * group
                    latent_ref[base : base + group, columns] = scaled[side * group : (side + 1) * group]
        latent = latent_ref[...]
        keys = jnp.dot(latent, key_w, preferred_element_type=F32).astype(BF16)
        values = lax.dot_general(
            value_w, latent, (((0,), (1,)), ((), ())), preferred_element_type=F32
        ).astype(BF16)
        rope = rope_ref[...]
        count = chunk * group
        spans = [slice(i * count, (i + 1) * count) for i in range(2)]
        heads = [slice(i * NOPE, (i + 1) * NOPE) for i in range(2)]
        scores = [
            jnp.concatenate(
                [dot_nt(jnp.concatenate([keys[span, head], rope], axis=1), query[i]) for head, query in zip(heads, queries)],
                axis=1,
            )
            for i, span in enumerate(spans)
        ]
        peak = jnp.max(jnp.maximum(*scores), axis=0, keepdims=True)
        if state is not None:
            peak = jnp.maximum(peak, state[0])
        weights = [jnp.exp(piece - peak) for piece in scores]
        total = jnp.sum(weights[0] + weights[1], axis=0, keepdims=True)
        weights = [piece.astype(BF16) for piece in weights]
        out = jnp.concatenate(
            [
                sum(
                    jnp.dot(values[head, span], weight[:, i * half : (i + 1) * half], preferred_element_type=F32)
                    for span, weight in zip(spans, weights)
                )
                for i, head in enumerate(heads)
            ],
            axis=1,
        )
        if state is not None:
            rescale = jnp.exp(state[0] - peak)
            total = total + state[1] * rescale
            out = out + state[2] * rescale
        return peak, total, out

    state = (stats_in[0:1], stats_in[1:2], out_in[...]) if stage > 0 else None
    if chunk == len(views[0][1]):
        peak, total, out = one_chunk(None, state)
    else:
        if state is None:
            state = (
                jnp.full((1, tokens), -jnp.inf, F32),
                jnp.zeros((1, tokens), F32),
                jnp.zeros((VDIM, tokens), F32),
            )
        steps = len(views[0][1]) // chunk
        peak, total, out = lax.fori_loop(0, steps, lambda i, state: one_chunk(i * chunk, state), state)
    if not last:
        stats_ref[0:1] = peak
        stats_ref[1:2] = total
        out_ref[...] = out
        return
    logs = peak + jnp.log(total)
    keep_log_ref[...] = logs[:, :half]
    send_log_ref[...] = logs[:, half:]
    out = out * (1.0 / total)
    rows = half // pairs
    result = None
    for i, weight_ref in enumerate((own_w_ref, other_w_ref)):
        attended = jnp.transpose(out[:, i * half : (i + 1) * half]).astype(BF16)
        both_ref[i, :, :VDIM] = attended
        both_ref[i, :, VDIM:] = query_refs[i][:, NOPE + LANES :]
        order = [both_ref[i, pl.ds(pl.multiple_of((chip ^ j) * rows, rows), rows), :] for j in range(pairs)]
        product = jnp.dot(jnp.concatenate(order, axis=0), weight_ref[: 2 * VDIM], preferred_element_type=F32)
        result = product if result is None else result + product
    for i, ref in enumerate(block_refs):
        ref[...] = result[i * rows : (i + 1) * rows].astype(ref.dtype)


def join_logs(own_ref, got_ref, log_ref):
    ranks = lax.axis_size("tp")
    rows = log_ref.shape[1] // ranks
    first = lax.axis_index("tp") % 2 == 0
    own, got = own_ref[...], got_ref[...]
    sides = [jnp.where(first, own, got), jnp.where(first, got, own)]
    lane = lax.broadcasted_iota(jnp.int32, log_ref.shape, 1) // rows
    logs = jnp.zeros(log_ref.shape, F32)
    for i in range(ranks):
        side = jnp.concatenate([sides[i % 2]] * 2, axis=1)
        shift = (i - i // 2) * rows
        logs = jnp.where(lane == i, pltpu.roll(side, shift, 1) if shift else side, logs)
    log_ref[...] = logs


def body(
    activations,
    norm_gain,
    query_weight,
    latent_weight,
    rope_key_weight,
    latent_gain,
    expand_weight,
    gate_weight,
    pre_weight,
    value_weight,
    conv_kernel,
    output_attend,
    output_conv,
):
    ranks = lax.axis_size("tp")
    places = lax.axis_size("sp")
    pairs = ranks // 2
    tokens, width = activations.shape
    features = ranks * width
    half = tokens // 2
    share = half // ranks
    rows = tokens // ranks
    channels = gate_weight.shape[1]

    even = [activations] + exchange(activations, "tp", 2, pairs)
    odd = swap_each(even)

    latent_t = latent_weight.T
    partner_t = swap(latent_t, "tp", 1)
    key_w, query_w, mix_w, own_w, cosines, sines = kernel_call(
        prepare,
        [
            ((4 * ROPE, features), BF16),
            ((NOPE + 2 * ROPE, features), BF16),
            ((features, 2 * LANES), BF16),
            ((VDIM + channels + expand_weight.size // features, features), BF16),
            ((tokens, LANES), F32),
            ((tokens, LANES), F32),
        ],
        16 << 20,
        scratch=[pltpu.SemaphoreType.DMA((9 + features // (NOPE + VDIM),))],
        flops=1 << 28,
        nbytes=1 << 23,
        in_hbm=range(8),
    )(
        latent_t, rope_key_weight.T, query_weight.T, pre_weight, value_weight, output_attend, output_conv,
        expand_weight, partner_t,
    )
    other_w = swap(own_w, "tp", 1)

    gain = norm_gain.reshape(1, -1)
    part = features // 2
    scaled_even, *partial = kernel_call(
        functools.partial(project_even, pairs),
        [((tokens, part), BF16), ((tokens, LANES), F32), ((tokens, 2 * LANES), F32), ((tokens, 2 * LANES), F32)],
        12 << 20,
        flops=2 * tokens * part * 4 * LANES,
        nbytes=4 * tokens * part,
    )(*even, gain, key_w, mix_w)
    scaled_odd, inv, message, mix = kernel_call(
        functools.partial(project_first, pairs),
        [
            ((tokens, part), BF16),
            ((tokens, LANES), F32),
            ((half + share + HALO, LANES), BF16),
            ((tokens, channels), BF16),
        ],
        12 << 20,
        scratch=[pltpu.VMEM((tokens, 2 * LANES), F32)],
        flops=2 * tokens * part * 4 * LANES,
        nbytes=4 * tokens * part,
    )(*odd, gain, key_w, mix_w, cosines, sines, *partial)

    small = places <= 8 and places & (places - 1) == 0
    if small:
        halos = [message] + exchange(message, "sp", 1, places)
        near = message[: half + share]
        nears = [near] + exchange(near, "tp", 2, pairs)
        near_other = swap(jnp.stack(nears), "tp", 1)
        around = jnp.stack([piece[: half + share] for piece in halos[1:]])
    else:
        around = lax.all_gather(message, "sp", axis=0)
        around, halos = around[:, : half + share], [around[:, half + share :]]
    arounds = [around] + exchange(around, "tp", 2, pairs)
    others = swap_each(arounds)
    slots = [[(i, k) for k in (range(places - 1) if small else range(places))] for i in range(pairs)]

    columns = NOPE + LANES + channels
    keep, send = kernel_call(
        functools.partial(project_second, not small),
        [((half, columns), BF16)] * 2,
        12 << 20,
        scratch=[pltpu.VMEM((tokens, columns), F32)],
        flops=2 * tokens * features * 3 * LANES,
        nbytes=4 * tokens * features,
    )(scaled_even, scaled_odd, inv, query_w, gate_weight, cosines, sines, mix, conv_kernel, *halos)
    got = swap(send, "tp", 1)

    def attend_to(arrays, slots, stage, outs, *state):
        chunk = len(slots[0]) if small else 4
        scratch = [
            pltpu.VMEM((2, half, VDIM + channels), BF16),
            pltpu.VMEM((chunk * half, pairs * LANES), BF16),
            pltpu.VMEM((chunk * half // 2, LANES), BF16),
        ]
        return kernel_call(
            functools.partial(attend, slots, chunk, stage),
            outs,
            (14 << 20) if small else (40 << 20),
            scratch=scratch if stage == 2 else scratch[1:],
            flops=1 << 29,
            nbytes=1 << 22,
        )(*arrays, latent_gain.reshape(1, -1), own_w, other_w, keep, got, *state)

    state_outs = [((8, tokens), F32), ((VDIM, tokens), F32)]
    first_slots, last_slots, first_in, last_in = slots, slots, arounds, others
    if small:
        first_slots = [[(pairs + i, None)] + chip_slots for i, chip_slots in enumerate(slots)]
        last_slots = [[(pairs, i)] + chip_slots for i, chip_slots in enumerate(slots)]
        first_in, last_in = arounds + nears, others + [near_other]
    state = attend_to(first_in, first_slots, 0, state_outs)
    final_outs = [((rows, features), F32)] + [((rows, features), BF16)] * (pairs - 1) + [((1, half), F32)] * 2
    *outs, own_log, send_log = attend_to(last_in, last_slots, 2, final_outs, *state)
    arrived = exchange_blocks(outs)
    got_log = swap(send_log, "tp", 1)
    (logs,) = kernel_call(join_logs, [((1, tokens), F32)], 1 << 20, flops=1 << 22, nbytes=1 << 12)(own_log, got_log)
    total = outs[0]
    for piece in arrived:
        total = total + piece.astype(F32)
    return total.astype(BF16), logs


def solution(mesh):
    return jax.shard_map(
        body,
        mesh=mesh,
        in_specs=(
            P("sp", "tp"),
            P(),
            P(None, "tp"),
            P(None, "tp"),
            P(),
            P(),
            P(None, "tp"),
            P(None, "tp"),
            P(None, "tp"),
            P(None, "tp"),
            P(None, "tp"),
            P("tp", None),
            P("tp", None),
        ),
        out_specs=(P(("sp", "tp"), None), P("tp", "sp")),
        check_vma=False,
    )
```

```python
import functools
import math

import jax
import jax.numpy as jnp
from jax import lax
from jax.experimental import pallas as pl
from jax.experimental.pallas import tpu as pltpu
from jax.sharding import PartitionSpec as P


NOPE = 128
ROPE = 64
VDIM = 128
GRID_W = 64
EPSILON = 1e-06
ROPE_BASE = 10000.0
LANES = 128
HALO = 8
F32 = jnp.float32
BF16 = jnp.bfloat16


def swap(array, axis, mask):
    peers = lax.axis_size(axis)
    return lax.ppermute(array, axis, [(i, i ^ mask) for i in range(peers)])


def exchange(array, axis, stride, peers):
    pieces = []
    for i in reversed(range(1, peers)):
        pieces.append(swap(array, axis, stride * i))
    return pieces[::-1]


def swap_each(arrays):
    pieces = []
    for array in arrays:
        pieces.append(swap(array, "tp", 1))
    return pieces


def exchange_blocks(blocks):
    arrived = []
    for i in reversed(range(1, len(blocks))):
        arrived.append(swap(blocks[i], "tp", 2 * i))
    return arrived


def kernel_call(body, outs, limit, scratch=(), flops=0, nbytes=0, in_hbm=()):
    whole = pl.BlockSpec(memory_space=pltpu.VMEM)

    def call(*operands):
        spaces = [pltpu.HBM if i in in_hbm else pltpu.VMEM for i in range(len(operands))]
        operands = [
            pltpu.with_memory_space_constraint(operand, space) if space is pltpu.HBM else operand
            for operand, space in zip(operands, spaces, strict=True)
        ]
        return pl.pallas_call(
            body,
            out_shape=[jax.ShapeDtypeStruct(shape, dtype) for shape, dtype in outs],
            in_specs=[pl.BlockSpec(memory_space=space) for space in spaces],
            out_specs=[whole] * len(outs),
            scratch_shapes=list(scratch),
            compiler_params=pltpu.CompilerParams(vmem_limit_bytes=limit),
            cost_estimate=pl.CostEstimate(flops=flops, bytes_accessed=nbytes, transcendentals=0),
        )(*operands)

    return call


def rotate(values, cosines, sines):
    quarter = ROPE // 4
    lane = lax.broadcasted_iota(jnp.int32, values.shape, 1)
    first = (lane // quarter) % 2 == 0
    ahead = pltpu.roll(values, LANES - quarter, 1)
    behind = pltpu.roll(values, quarter, 1)
    return values * cosines + jnp.where(first, ahead, behind) * sines


def low_lanes(shape):
    return lax.broadcasted_iota(jnp.int32, shape, 1) < ROPE


def prepare(
    latent_ref, rope_ref, query_ref, pre_ref, value_ref, attend_ref, conv_ref, expand_ref, partner_ref,
    key_w_ref, query_w_ref, mix_w_ref, own_w_ref, cos_ref, sin_ref, expand_in, sems,
):
    core = lax.axis_index("tp") % 2
    mine = pl.ds(pl.multiple_of(core * ROPE, ROPE), ROPE)
    moves = [
        (latent_ref, key_w_ref.at[mine]),
        (rope_ref, key_w_ref.at[2 * ROPE : 3 * ROPE]),
        (rope_ref, key_w_ref.at[3 * ROPE :]),
        (pre_ref, mix_w_ref.at[:, :LANES]),
        (value_ref, mix_w_ref.at[:, LANES:]),
        (query_ref, query_w_ref.at[: NOPE + ROPE]),
        (query_ref.at[NOPE:], query_w_ref.at[NOPE + ROPE :]),
        (attend_ref, own_w_ref.at[:VDIM]),
        (conv_ref, own_w_ref.at[VDIM : 2 * VDIM]),
    ]
    moves.append((expand_ref, expand_in))
    copies = [pltpu.make_async_copy(source, target, sems.at[i]) for i, (source, target) in enumerate(moves)]
    for copy in copies:
        copy.start()
    key_w_ref[pl.ds(pl.multiple_of((1 - core) * ROPE, ROPE), ROPE), :] = partner_ref[...]
    quarter = ROPE // 4
    groups = cos_ref.shape[0] // GRID_W
    first_row = lax.axis_index("sp") * groups

    def angles(rows, start):
        lane = lax.broadcasted_iota(jnp.int32, (rows, LANES), 1) % ROPE
        place = (lax.broadcasted_iota(jnp.int32, (rows, LANES), 0) + start).astype(F32)
        inverse = jnp.exp((lane % quarter).astype(F32) * (-math.log(ROPE_BASE) / quarter))
        angle = place * inverse
        sign = jnp.where((lane // quarter) % 2 == 0, -1.0, 1.0)
        return lane < 2 * quarter, jnp.cos(angle), jnp.sin(angle) * sign

    _, row_cos, row_sin = angles(groups, first_row)
    by_row, col_cos, col_sin = angles(GRID_W, 0)
    for g in range(groups):
        rows = slice(g * GRID_W, (g + 1) * GRID_W)
        cos_ref[rows, :] = jnp.where(by_row, row_cos[g : g + 1], col_cos)
        sin_ref[rows, :] = jnp.where(by_row, row_sin[g : g + 1], col_sin)
    for copy in copies:
        copy.wait()
    high, deep = own_w_ref.shape[0] - 2 * VDIM, expand_in.shape[0]
    turned = jnp.transpose(expand_in[...].astype(F32)).astype(BF16)
    for k in range(own_w_ref.shape[1] // deep):
        own_w_ref[2 * VDIM :, k * deep : (k + 1) * deep] = turned[k * high : (k + 1) * high]


def dot_nt(left, right):
    return lax.dot_general(left, right, (((1,), (1,)), ((), ())), preferred_element_type=F32)


def weights_for(ref, owners, width, axis):
    spans = [pl.ds(pl.multiple_of(owner * width, width), width) for owner in owners]
    return jnp.concatenate([ref[:, span] if axis else ref[span, :] for span in spans], axis=axis)


def owners_of(core, pairs):
    return [lax.axis_index("tp") ^ (2 * i + core) for i in range(pairs)]


def project(core, pieces, gain_ref, key_w_ref, mix_w_ref, scaled_ref):
    owners = owners_of(core, len(pieces))
    tokens, width = pieces[0].shape
    total = jnp.zeros((tokens, LANES), F32)
    for i, (owner, ref) in enumerate(zip(owners, pieces)):
        piece = ref[...].astype(F32)
        squares = piece * piece
        for j in range(width // LANES):
            total = total + squares[:, j * LANES : (j + 1) * LANES]
        gain = gain_ref[:, pl.ds(pl.multiple_of(owner * width, width), width)]
        scaled_ref[:, i * width : (i + 1) * width] = (piece * gain).astype(BF16)
    scaled = scaled_ref[...]
    keys = dot_nt(scaled, weights_for(key_w_ref, owners, width, 1))
    mixes = jnp.dot(scaled, weights_for(mix_w_ref, owners, width, 0), preferred_element_type=F32)
    return total, keys, mixes


def project_even(pairs, *refs):
    pieces, (gain_ref, key_w_ref, mix_w_ref, scaled_ref, total_ref, keys_ref, mixes_ref) = refs[:pairs], refs[pairs:]
    total, keys, mixes = project(0, pieces, gain_ref, key_w_ref, mix_w_ref, scaled_ref)
    total_ref[...] = total
    keys_ref[...] = keys
    mixes_ref[...] = mixes


def project_first(pairs, *refs):
    pieces, refs = refs[:pairs], refs[pairs:]
    gain_ref, key_w_ref, mix_w_ref, cos_ref, sin_ref, total_ref, keys_ref, mixes_ref = refs[:8]
    scaled_ref, inv_ref, message_ref, mix_ref, key_ref = refs[8:]
    total, keys, mixes = project(1, pieces, gain_ref, key_w_ref, mix_w_ref, scaled_ref)
    rank = lax.axis_index("tp")
    tokens, width = pieces[0].shape
    half = tokens // 2
    features = 2 * pairs * width
    total = jnp.sum(total + total_ref[...], axis=1, keepdims=True)
    inv = lax.rsqrt(total / features + EPSILON)
    inv_ref[...] = jnp.broadcast_to(inv, inv_ref.shape)
    keys = (keys + keys_ref[...]) * inv
    mixes = (mixes + mixes_ref[...]) * inv
    mix = (mixes[:, :LANES] * mixes[:, LANES:]).astype(BF16)
    mix_ref[...] = mix
    key_ref[...] = keys
    chip, core = rank // 2, rank % 2
    start = pl.multiple_of(core * half, half)
    message_ref[:half, :] = key_ref[pl.ds(start, half), :LANES].astype(BF16)
    share = half // (2 * pairs)
    turned = []
    for base in (0, half // 2):
        rows = pl.ds(pl.multiple_of(start + base + chip * share, share), share)
        turned.append(rotate(key_ref[rows, LANES:], cos_ref[rows, :], sin_ref[rows, :]))
    low = low_lanes((share, LANES))
    message_ref[half : half + share, :] = jnp.where(low, turned[0], turned[1]).astype(BF16)
    row = lax.broadcasted_iota(jnp.int32, (HALO, LANES), 0)
    first = jnp.broadcast_to(mix[:1].astype(F32), (HALO, LANES))
    last = jnp.broadcast_to(mix[tokens - 1 :].astype(F32), (HALO, LANES))
    message_ref[half + share :, :] = jnp.where(row == 0, first, last).astype(BF16)


def project_second(natural, *refs):
    even_ref, odd_ref, inv_ref, query_w_ref, gate_w_ref, cos_ref, sin_ref, mix_ref, taps_ref = refs[:9]
    halos, (keep_ref, send_ref, both_ref) = refs[9:-3], refs[-3:]
    pairs = lax.axis_size("tp") // 2
    width = even_ref.shape[1] // pairs
    owners = owners_of(0, pairs) + owners_of(1, pairs)
    scaled = jnp.concatenate([even_ref[...], odd_ref[...]], axis=1)
    inv = inv_ref[...]
    scale = (NOPE + ROPE) ** (-0.5)
    query = dot_nt(scaled, weights_for(query_w_ref, owners, width, 1))
    both_ref[:, :NOPE] = query[:, :NOPE] * inv * scale
    both_ref[:, NOPE : NOPE + LANES] = rotate(query[:, NOPE:] * inv, cos_ref[...], sin_ref[...]) * scale

    gate = jnp.dot(scaled, weights_for(gate_w_ref, owners, width, 0), preferred_element_type=F32) * inv
    mix = mix_ref[...].astype(F32)
    tokens = mix.shape[0]
    place, places = lax.axis_index("sp"), lax.axis_size("sp")

    def edge_of(other, at):
        inside = (other >= 0) & (other < places)
        other = jnp.clip(other, 0, places - 1)
        if natural:
            edges = halos[0][other].astype(F32)
        else:
            edges = jnp.zeros((HALO, LANES), F32)
            for i, ref in enumerate(halos):
                edges = jnp.where((other ^ place) == i, ref[ref.shape[0] - HALO :, :].astype(F32), edges)
        return jnp.where(inside, edges[at : at + 1, :], 0.0)

    row = lax.broadcasted_iota(jnp.int32, mix.shape, 0)
    earlier = jnp.where(row == 0, edge_of(place - 1, 1), pltpu.roll(mix, 1, 0))
    later = jnp.where(row == tokens - 1, edge_of(place + 1, 0), pltpu.roll(mix, tokens - 1, 0))
    taps = taps_ref[...].astype(F32)
    convolved = taps[0:1] * earlier + taps[1:2] * mix + taps[2:3] * later
    both_ref[:, NOPE + LANES :] = gate * convolved
    core = lax.axis_index("tp") % 2
    rows = tokens // lax.axis_size("tp")
    for i in range(lax.axis_size("tp") // 2):
        for ref, side in ((keep_ref, core), (send_ref, 1 - core)):
            source = pl.ds(pl.multiple_of((2 * i + side) * rows, rows), rows)
            ref[i * rows : (i + 1) * rows, :] = both_ref[source, :].astype(BF16)


def attend(slots, chunk, stage, *refs):
    inputs = 1 + max(place for chip_slots in slots for place, _ in chip_slots)
    pieces, refs = refs[:inputs], refs[inputs:]
    gain_ref, own_w_ref, other_w_ref, query_refs = refs[0], refs[1], refs[2], refs[3:5]
    refs = refs[5:]
    if stage > 0:
        stats_in, out_in = refs[:2]
        refs = refs[2:]
    last = stage == 2
    if last:
        block_refs, (keep_log_ref, send_log_ref, both_ref) = refs[:-5], refs[-5:-2]
    else:
        stats_ref, out_ref = refs[:2]
    latent_ref, rope_ref = refs[-2:]
    rank = lax.axis_index("tp")
    chip = rank // 2
    pairs = len(slots)
    half = query_refs[0].shape[0]
    tokens = 2 * half
    group = half // 2
    share = group // pairs
    entries = pairs * LANES

    low = low_lanes((half, LANES))
    queries = []
    for ref in query_refs:
        nope, rope = ref[:, :NOPE], ref[:, NOPE : NOPE + LANES]
        zeros = jnp.zeros_like(rope)
        sides = (jnp.where(low, rope, zeros), jnp.where(low, zeros, rope))
        queries.append([jnp.concatenate([nope, side], axis=1) for side in sides])
    deep = pairs * LANES
    blocks = range(own_w_ref.shape[1] // deep)

    def expansion(part):
        rows = [ref[2 * VDIM :, k * deep : (k + 1) * deep] for ref in (own_w_ref, other_w_ref) for k in part]
        return jnp.concatenate(rows, axis=0)

    key_w = expansion(blocks[: len(blocks) // 2])
    value_w = expansion(blocks[len(blocks) // 2 :])
    views = [(chip ^ i, chip_slots) for i, chip_slots in enumerate(slots)]

    def rows_of(chip_slots, slot, first, start, count):
        place, at = chip_slots[slot if first is None else 0]
        at = at if first is None else first + slot
        rows = slice(start, start + count)
        return pieces[place][rows, :] if at is None else pieces[place][at, rows, :]

    def one_chunk(first, state):
        for slot in range(chunk):
            total = jnp.zeros((half, LANES), F32)
            for owner, chip_slots in views:
                piece = rows_of(chip_slots, slot, first, 0, half).astype(F32)
                total = total + piece * piece
                start = pl.multiple_of(slot * group + owner * share, share)
                rope_ref[pl.ds(start, share), :] = rows_of(chip_slots, slot, first, half, share)
            inv = lax.rsqrt(jnp.sum(total, axis=1, keepdims=True) / entries + EPSILON)
            for owner, chip_slots in views:
                piece = rows_of(chip_slots, slot, first, 0, half).astype(F32)
                columns = pl.ds(pl.multiple_of(owner * LANES, LANES), LANES)
                scaled = (piece * inv * gain_ref[:, columns]).astype(BF16)
                for side in range(2):
                    base = (side * chunk + slot) * group
                    latent_ref[base : base + group, columns] = scaled[side * group : (side + 1) * group]
        latent = latent_ref[...]
        keys = dot_nt(latent, key_w).astype(BF16)
        values = dot_nt(value_w, latent).astype(BF16)
        rope = rope_ref[...]
        count = chunk * group
        spans = [slice(i * count, (i + 1) * count) for i in range(2)]
        heads = [slice(i * NOPE, (i + 1) * NOPE) for i in range(2)]
        scores = [
            jnp.concatenate(
                [dot_nt(jnp.concatenate([keys[span, head], rope], axis=1), query[i]) for head, query in zip(heads, queries)],
                axis=1,
            )
            for i, span in enumerate(spans)
        ]
        peak = jnp.max(jnp.maximum(*scores), axis=0, keepdims=True)
        if state is not None:
            peak = jnp.maximum(peak, state[0])
        weights = [jnp.exp(piece - peak) for piece in scores]
        total = jnp.sum(weights[0] + weights[1], axis=0, keepdims=True)
        weights = [piece.astype(BF16) for piece in weights]
        out = jnp.concatenate(
            [
                sum(
                    jnp.dot(values[head, span], weight[:, i * half : (i + 1) * half], preferred_element_type=F32)
                    for span, weight in zip(spans, weights)
                )
                for i, head in enumerate(heads)
            ],
            axis=1,
        )
        if state is not None:
            rescale = jnp.exp(state[0] - peak)
            total = total + state[1] * rescale
            out = out + state[2] * rescale
        return peak, total, out

    state = (stats_in[0:1], stats_in[1:2], out_in[...]) if stage > 0 else None
    if chunk == len(views[0][1]):
        peak, total, out = one_chunk(None, state)
    else:
        if state is None:
            state = (
                jnp.full((1, tokens), -jnp.inf, F32),
                jnp.zeros((1, tokens), F32),
                jnp.zeros((VDIM, tokens), F32),
            )
        steps = len(views[0][1]) // chunk
        peak, total, out = lax.fori_loop(0, steps, lambda i, state: one_chunk(i * chunk, state), state)
    if not last:
        stats_ref[0:1] = peak
        stats_ref[1:2] = total
        out_ref[...] = out
        return
    logs = peak + jnp.log(total)
    keep_log_ref[...] = logs[:, :half]
    send_log_ref[...] = logs[:, half:]
    out = out * (1.0 / total)
    rows = half // pairs
    result = None
    for i, weight_ref in enumerate((own_w_ref, other_w_ref)):
        attended = jnp.transpose(out[:, i * half : (i + 1) * half]).astype(BF16)
        both_ref[i, :, :VDIM] = attended
        both_ref[i, :, VDIM:] = query_refs[i][:, NOPE + LANES :]
        order = [both_ref[i, pl.ds(pl.multiple_of((chip ^ j) * rows, rows), rows), :] for j in range(pairs)]
        product = jnp.dot(jnp.concatenate(order, axis=0), weight_ref[: 2 * VDIM], preferred_element_type=F32)
        result = product if result is None else result + product
    for i, ref in enumerate(block_refs):
        ref[...] = result[i * rows : (i + 1) * rows].astype(ref.dtype)


def join_logs(own_ref, got_ref, log_ref):
    ranks = lax.axis_size("tp")
    rows = log_ref.shape[1] // ranks
    first = lax.axis_index("tp") % 2 == 0
    own, got = own_ref[...], got_ref[...]
    sides = [jnp.where(first, own, got), jnp.where(first, got, own)]
    lane = lax.broadcasted_iota(jnp.int32, log_ref.shape, 1) // rows
    logs = jnp.zeros(log_ref.shape, F32)
    for i in range(ranks):
        side = jnp.concatenate([sides[i % 2]] * 2, axis=1)
        shift = (i - i // 2) * rows
        logs = jnp.where(lane == i, pltpu.roll(side, shift, 1) if shift else side, logs)
    log_ref[...] = logs


def body(
    activations,
    norm_gain,
    query_weight,
    latent_weight,
    rope_key_weight,
    latent_gain,
    expand_weight,
    gate_weight,
    pre_weight,
    value_weight,
    conv_kernel,
    output_attend,
    output_conv,
):
    ranks = lax.axis_size("tp")
    places = lax.axis_size("sp")
    pairs = ranks // 2
    tokens, width = activations.shape
    features = ranks * width
    half = tokens // 2
    share = half // ranks
    rows = tokens // ranks
    channels = gate_weight.shape[1]

    even = [activations] + exchange(activations, "tp", 2, pairs)
    odd = swap_each(even)

    latent_t = latent_weight.T
    partner_t = swap(latent_t, "tp", 1)
    key_w, query_w, mix_w, own_w, cosines, sines = kernel_call(
        prepare,
        [
            ((4 * ROPE, features), BF16),
            ((NOPE + 2 * ROPE, features), BF16),
            ((features, 2 * LANES), BF16),
            ((VDIM + channels + expand_weight.size // features, features), BF16),
            ((tokens, LANES), F32),
            ((tokens, LANES), F32),
        ],
        16 << 20,
        scratch=[pltpu.VMEM(expand_weight.shape, BF16), pltpu.SemaphoreType.DMA((10,))],
        flops=1 << 28,
        nbytes=1 << 23,
        in_hbm=range(8),
    )(
        latent_t, rope_key_weight.T, query_weight.T, pre_weight, value_weight, output_attend, output_conv,
        expand_weight, partner_t,
    )
    other_w = swap(own_w, "tp", 1)

    gain = norm_gain.reshape(1, -1)
    part = features // 2
    scaled_even, *partial = kernel_call(
        functools.partial(project_even, pairs),
        [((tokens, part), BF16), ((tokens, LANES), F32), ((tokens, 2 * LANES), F32), ((tokens, 2 * LANES), F32)],
        12 << 20,
        flops=2 * tokens * part * 4 * LANES,
        nbytes=4 * tokens * part,
    )(*even, gain, key_w, mix_w)
    scaled_odd, inv, message, mix = kernel_call(
        functools.partial(project_first, pairs),
        [
            ((tokens, part), BF16),
            ((tokens, LANES), F32),
            ((half + share + HALO, LANES), BF16),
            ((tokens, channels), BF16),
        ],
        12 << 20,
        scratch=[pltpu.VMEM((tokens, 2 * LANES), F32)],
        flops=2 * tokens * part * 4 * LANES,
        nbytes=4 * tokens * part,
    )(*odd, gain, key_w, mix_w, cosines, sines, *partial)

    small = places <= 8 and places & (places - 1) == 0
    if small:
        halos = [message] + exchange(message, "sp", 1, places)
        near = message[: half + share]
        nears = [near] + exchange(near, "tp", 2, pairs)
        near_other = swap(jnp.stack(nears), "tp", 1)
        around = jnp.stack([piece[: half + share] for piece in halos[1:]])
    else:
        around = lax.all_gather(message, "sp", axis=0)
        around, halos = around[:, : half + share], [around[:, half + share :]]
    arounds = [around] + exchange(around, "tp", 2, pairs)
    others = swap_each(arounds)
    slots = [[(i, k) for k in (range(places - 1) if small else range(places))] for i in range(pairs)]

    columns = NOPE + LANES + channels
    keep, send = kernel_call(
        functools.partial(project_second, not small),
        [((half, columns), BF16)] * 2,
        12 << 20,
        scratch=[pltpu.VMEM((tokens, columns), F32)],
        flops=2 * tokens * features * 3 * LANES,
        nbytes=4 * tokens * features,
    )(scaled_even, scaled_odd, inv, query_w, gate_weight, cosines, sines, mix, conv_kernel, *halos)
    got = swap(send, "tp", 1)

    def attend_to(arrays, slots, stage, outs, *state):
        chunk = len(slots[0]) if small else 4
        scratch = [
            pltpu.VMEM((2, half, VDIM + channels), BF16),
            pltpu.VMEM((chunk * half, pairs * LANES), BF16),
            pltpu.VMEM((chunk * half // 2, LANES), BF16),
        ]
        return kernel_call(
            functools.partial(attend, slots, chunk, stage),
            outs,
            (14 << 20) if small else (40 << 20),
            scratch=scratch if stage == 2 else scratch[1:],
            flops=1 << 29,
            nbytes=1 << 22,
        )(*arrays, latent_gain.reshape(1, -1), own_w, other_w, keep, got, *state)

    state_outs = [((8, tokens), F32), ((VDIM, tokens), F32)]
    first_slots, last_slots, first_in, last_in = slots, slots, arounds, others
    if small:
        first_slots = [[(pairs + i, None)] + chip_slots for i, chip_slots in enumerate(slots)]
        last_slots = [[(pairs, i)] + chip_slots for i, chip_slots in enumerate(slots)]
        first_in, last_in = arounds + nears, others + [near_other]
    state = attend_to(first_in, first_slots, 0, state_outs)
    final_outs = [((rows, features), F32)] + [((rows, features), BF16)] * (pairs - 1) + [((1, half), F32)] * 2
    *outs, own_log, send_log = attend_to(last_in, last_slots, 2, final_outs, *state)
    arrived = exchange_blocks(outs)
    got_log = swap(send_log, "tp", 1)
    (logs,) = kernel_call(join_logs, [((1, tokens), F32)], 1 << 20, flops=1 << 22, nbytes=1 << 12)(own_log, got_log)
    total = outs[0]
    for piece in arrived:
        total = total + piece.astype(F32)
    return total.astype(BF16), logs


def solution(mesh):
    return jax.shard_map(
        body,
        mesh=mesh,
        in_specs=(
            P("sp", "tp"),
            P(),
            P(None, "tp"),
            P(None, "tp"),
            P(),
            P(),
            P(None, "tp"),
            P(None, "tp"),
            P(None, "tp"),
            P(None, "tp"),
            P(None, "tp"),
            P("tp", None),
            P("tp", None),
        ),
        out_specs=(P(("sp", "tp"), None), P("tp", "sp")),
        check_vma=False,
    )
```
